32 devices in a mesh: ep: 8 (over z, x), tp: 4 (over y, core).
Axes of the slice: x: 2, y: 2, z: 4, core: 2. Of those that a mesh axis runs over, the one named last changes fastest.
Arguments:
- blender_incoming_features: bfloat16 [2048, 4096], P('ep', 'tp'), may hold values from -6 to 6
- entry_latent_matrix: bfloat16 [2048, 2048], P('ep', 'tp'), may hold values from -6 to 6
- exit_latent_matrix: bfloat16 [2048, 2048], P('ep', 'tp'), may hold values from -6 to 6
- unactivated_valve: bfloat16 [2048, 4096], P('ep', 'tp'), may hold values from -6 to 6
- presoftplus_strides: float32 [2048, 64], P('ep', 'tp'), may hold values from -7 to 7
- extra_attenuation: float32 [2048, 64], P('ep', 'tp'), may hold values from -1 to 0
- incoming_feature_kernel: bfloat16 [4, 4096], P(None, 'tp'), may hold values from -3 to 3
- entry_latent_kernel: bfloat16 [4, 2048], P(None, 'tp'), may hold values from -3 to 3
- exit_latent_kernel: bfloat16 [4, 2048], P(None, 'tp'), may hold values from -3 to 3
- stride_offset_vector: float32 [64], P('tp'), may hold values from -1 to 1
- attenuation_speed_exponent: float32 [64], P('tp'), may hold values from -16 to -3
- bypass_coef_vector: float32 [64], P('tp'), may hold values from 0.5 to 4
- cluster_rescale_coefs: bfloat16 [4096], P('tp'), may hold values from 0.099609375 to 1.8984375
- blender_result_matrix: bfloat16 [4096, 2048], P('tp'), may hold values from -0.09375 to 0.09375
- latter_microbatch_activations: bfloat16 [2048, 2048], P('ep'), may hold values from -6 to 6
- specialist_rescale_coefs: bfloat16 [2048], replicated, may hold values from 0.099609375 to 1.8984375
- specialist_valve_matrix: bfloat16 [8, 2048, 4096], P('ep', None, 'tp'), may hold values from -0.125 to 0.125
- specialist_expand_matrix: bfloat16 [8, 2048, 4096], P('ep', None, 'tp'), may hold values from -0.125 to 0.125
- specialist_contract_matrix: bfloat16 [8, 4096, 2048], P('ep', 'tp'), may hold values from -0.125 to 0.125
- specialist_picks: int32 [2048, 2], P('ep'), may hold values from 0 to 7, all different within a row; in each aligned block of 256 rows (0 to 255, 256 to 511, ...) at most 96 rows name the same one
- selected_specialist_coefs: float32 [2048, 2], P('ep'), may hold values from 0.1 to 1
Outputs:
- mixed_a: bfloat16 [2048, 2048], P(('ep', 'tp'))
- mixed_b: bfloat16 [2048, 2048], P('ep', 'tp')
The draws below stay inside these ranges and needn't reach their ends.
Inputs may be any that keep to these rules, and one draw needn't show every extreme that they name: `specialist_picks`: in each aligned block of 256 rows, the rows of one index of ep, no expert is named by more than 96 rows, a bound that some block reaches.
All inputs are finite; a program needn't handle non-finite values.
Results may differ from the reference program's by a relative error of at most 0.019.
Values may be sent and summed in bfloat16 or wider, within the bound.
A program may use at most 64 MiB of HBM per device.

```python
import math
import jax
import jax.numpy as jnp
import numpy as np
from jax import lax

D = 2048
HEADS = 64
HEAD_DIM = 64
SHARING_CLUSTERS = 16
STATE = 128
CONV = 4
BLOCK = 64
FF = 4096
TOPK = 2
TOK_B_DEV = 256
INNER = 4096
EXPERTS = 8
SEQ_A = 2048
TOKENS_B = 2048
CAP = 96
N_EP = 8
N_TP = 4


def draw_presoftplus_strides(key, part):
    base_key, shift_key = jax.random.split(jax.random.fold_in(key, 3))
    base_draw = jnp.clip(jax.random.normal(base_key, (SEQ_A, HEADS), jnp.float32), -6.0, 6.0)
    offsets = jax.random.uniform(shift_key, (SEQ_A // BLOCK, 1), jnp.float32, -0.8, 0.8)
    return base_draw + jnp.repeat(offsets, BLOCK, axis=0)


def draw_attenuation_speed_exponent(key, part):
    pick_key, slow_key, fast_key = jax.random.split(jax.random.fold_in(key, 7), 3)
    slow_share = 50
    is_slow = jax.random.randint(pick_key, (HEADS,), 0, 100) < slow_share
    slow_rates = jax.random.uniform(slow_key, (HEADS,), jnp.float32, math.log(0.05 / SEQ_A), math.log(0.4 / SEQ_A))
    fast_rates = jax.random.uniform(fast_key, (HEADS,), jnp.float32, math.log(0.01), math.log(0.035))
    return jnp.where(is_slow, slow_rates, fast_rates)


def draw_extra_attenuation(key, part):
    place_key, factor_key = jax.random.split(jax.random.fold_in(key, 13))
    word_locations = jax.random.randint(place_key, (2,), 0, SEQ_A)
    multiplier_entries = jax.random.uniform(factor_key, (HEADS,), jnp.float32, math.log(0.55), math.log(0.8))
    line_ordinal_array = jnp.arange(SEQ_A)
    spike_marker = jnp.any(line_ordinal_array[:, None] == word_locations[None, :], axis=1)
    return jnp.where(spike_marker[:, None], multiplier_entries[None, :], jnp.zeros((), jnp.float32))


def spiked(entries, stream_key, source, target, parts, factor):
    owner, partner = [(jnp.arange(entries.shape[position]) // (entries.shape[position] // parts)).reshape([-1 if axis == position else 1 for axis in range(entries.ndim)]) for position in (source, target)]
    chosen = jax.random.permutation(stream_key, parts)[partner]
    strong = (owner == chosen) | (owner == (partner + parts // 2) % parts)
    return jnp.where(strong, factor * entries, entries)


def shard_levels(own_key, dims, cuts, low, high):
    gain, own = 1.0, jax.random.fold_in(own_key, 6)
    for dim, parts in cuts:
        steps = jnp.exp(jax.random.uniform(jax.random.fold_in(own, dim), (parts,), jnp.float32, low / len(cuts), high / len(cuts)))
        gain = gain * jnp.repeat(steps, dims[dim] // parts).reshape([-1 if axis == dim else 1 for axis in range(len(dims))])
    return gain


def assign_block(stream_key, own, number, rows, number_of, top, limit, skew):
    order = jax.random.permutation(stream_key, number_of)
    crowded, common = portions_of(number_of, rows * top, limit, skew, True), portions_of(number_of, rows * top, limit, skew, False)
    places = jnp.arange(number_of)

    def named(tallies, rotation):
        used = int((tallies > 0).sum())
        fixed = max(1, used // 4)
        moved = fixed + (places - fixed + rotation * (used - fixed)) % max(1, number_of - fixed)
        return jnp.zeros((number_of,), jnp.int32).at[order[jnp.where(places < fixed, places, moved)]].set(jnp.asarray(tallies, jnp.int32))

    tallies = jnp.where(number % 4 == 0, named(crowded, number // 4), named(common, number - number // 4 - 1))
    mixed = jax.random.permutation(jax.random.fold_in(own, 3), number_of)
    giver, receiver = mixed[0:number_of // 2 * 2:2], mixed[1:number_of // 2 * 2:2]
    margin = jnp.minimum(tallies[giver] - 1, limit - tallies[receiver]) // 2
    margin = jnp.where((giver == order[0]) | (receiver == order[0]) | (tallies[receiver] == 0), 0, jnp.maximum(margin, 0))
    moved = jax.random.randint(jax.random.fold_in(own, 4), (number_of // 2,), 0, 1 << 20) % (margin + 1)
    tallies = tallies.at[giver].add(-moved).at[receiver].add(moved)
    items = jnp.searchsorted(jnp.cumsum(tallies), jnp.arange(rows * top), side="right").astype(jnp.int32)
    grid = items.reshape(top, rows).T
    grid = grid[jax.random.permutation(jax.random.fold_in(own, 1), rows)]
    rotation = jax.random.randint(jax.random.fold_in(own, 2), (rows, 1), 0, top)
    return jnp.take_along_axis(grid, (jnp.arange(top)[None, :] + rotation) % top, axis=1)


def portions_of(count, total, reach, skew, full):
    portions = [(1 << 20) // math.isqrt(standing ** skew) + 1 for standing in range(1, count + 1)]
    largest = reach if full else min(reach, max(-(-total // count), total * portions[0] // sum(portions)))
    least = 1 if total - largest >= count - 1 else 0
    given, surplus = [largest] + [least] * (count - 1), total - largest - least * (count - 1)
    while surplus > 0:
        movable = [i for i in range(1, count) if given[i] < largest] or [i for i in range(1, count) if given[i] < reach]
        pool, remaining = sum([portions[i] for i in movable]), surplus
        for i in movable:
            extra = min(reach - given[i], max(1, remaining * portions[i] // pool), surplus)
            given[i] = given[i] + extra
            surplus = surplus - extra
    return np.array(given)


def scatter_about(own_key, shape, width, bound, shards=(), held_as=jnp.bfloat16):
    result = jax.random.normal(own_key, shape, jnp.float32) * width
    if len(shards) > 0:
        result = shard_levels(own_key, shape, shards, -0.22, 0.18) * result
    return jnp.clip(result, min=-bound, max=bound).astype(held_as)


def noise_with(key, extent, deviation, limit, cuts, heavy, kind=jnp.bfloat16):
    entries = deviation * jax.random.normal(key, extent, jnp.float32)
    if cuts:
        entries = entries * shard_levels(key, extent, cuts, -0.22, 0.18)
    return jnp.clip(spiked(entries, jax.random.fold_in(key, 3), *heavy), -limit, limit).astype(kind)


def setup_inputs(seed: int = 0) -> dict:
    streams_of = jax.random.split(jax.random.key(seed), 22)
    blender_incoming_features = scatter_about(streams_of[0], (SEQ_A, INNER), 1.0, 6.0, ((0, 8), (1, 4)))
    entry_latent_matrix = scatter_about(streams_of[1], (SEQ_A, SHARING_CLUSTERS * STATE), 1.0, 6.0, ((0, 8), (1, 4)))
    exit_latent_matrix = scatter_about(streams_of[2], (SEQ_A, SHARING_CLUSTERS * STATE), 1.0, 6.0, ((0, 8), (1, 4)))
    unactivated_valve = scatter_about(streams_of[3], (SEQ_A, INNER), 1.0, 6.0, ((0, 8), (1, 4)))
    presoftplus_strides = draw_presoftplus_strides(jax.random.fold_in(streams_of[21], 71), 0)
    extra_attenuation = draw_extra_attenuation(jax.random.fold_in(streams_of[21], 71), 0)
    incoming_feature_kernel = scatter_about(streams_of[6], (CONV, INNER), CONV ** -0.5, 3.0, ((1, 4),))
    entry_latent_kernel = scatter_about(streams_of[7], (CONV, SHARING_CLUSTERS * STATE), CONV ** -0.5, 3.0, ((1, 4),))
    exit_latent_kernel = scatter_about(streams_of[8], (CONV, SHARING_CLUSTERS * STATE), CONV ** -0.5, 3.0, ((1, 4),))
    stride_offset_vector = jnp.clip(jax.random.uniform(streams_of[9], (HEADS,), jnp.float32, -1.0, 1.0) * shard_levels(streams_of[9], (HEADS,), ((0, 4),), -0.4, 0.0), -1.0, 1.0)
    attenuation_speed_exponent = draw_attenuation_speed_exponent(jax.random.fold_in(streams_of[21], 71), 0)
    bypass_coef_vector = jnp.clip(jnp.exp(math.log(4.0) - 2.0794415 * jax.random.uniform(streams_of[11], (HEADS,), jnp.float32) ** shard_levels(streams_of[11], (HEADS,), ((0, 4),), -0.2, 0.2)), 0.5, 4.0)
    cluster_rescale_coefs = jnp.clip(1.0 + 0.18 * jax.random.normal(streams_of[12], (INNER,), jnp.float32), 0.099609375, 1.8984375).astype(jnp.bfloat16)
    blender_result_matrix = scatter_about(streams_of[13], (INNER, D), INNER ** -0.5, 0.09375, ((0, 4),))
    latter_microbatch_activations = scatter_about(streams_of[14], (TOKENS_B, D), 1.0, 6.0, ((0, 8),))
    specialist_rescale_coefs = jnp.clip(1.0 + 0.18 * jax.random.normal(streams_of[15], (D,), jnp.float32), 0.099609375, 1.8984375).astype(jnp.bfloat16)
    specialist_valve_matrix = scatter_about(streams_of[16], (EXPERTS, D, FF), D ** -0.5, 0.125, ((0, 8), (2, 4)))
    specialist_expand_matrix = scatter_about(streams_of[17], (EXPERTS, D, FF), D ** -0.5, 0.125, ((0, 8), (2, 4)))
    specialist_contract_matrix = noise_with(streams_of[18], (EXPERTS, FF, D), FF ** -0.5, 0.125, ((0, 8), (1, 4)), (1, 2, 4, 2.0))
    specialist_picks_keys = jax.random.split(jax.random.fold_in(streams_of[19], 1), TOKENS_B // TOK_B_DEV)
    specialist_picks_turns = jax.random.permutation(jax.random.fold_in(streams_of[19], 3), TOKENS_B // TOK_B_DEV)
    specialist_picks = jax.vmap(lambda own, number: assign_block(jax.random.fold_in(streams_of[19], 2), own, number, TOK_B_DEV, EXPERTS, TOPK, CAP, 2))(specialist_picks_keys, specialist_picks_turns).reshape((TOKENS_B, TOPK))
    selected_specialist_coefs = jnp.clip(0.1 + 0.9 * jax.random.uniform(streams_of[20], (TOKENS_B, TOPK), jnp.float32) ** shard_levels(streams_of[20], (TOKENS_B, TOPK), ((0, 8),), -0.2, 0.2), 0.1, 1.0)
    return {"blender_incoming_features": blender_incoming_features, "entry_latent_matrix": entry_latent_matrix, "exit_latent_matrix": exit_latent_matrix, "unactivated_valve": unactivated_valve, "presoftplus_strides": presoftplus_strides, "extra_attenuation": extra_attenuation, "incoming_feature_kernel": incoming_feature_kernel, "entry_latent_kernel": entry_latent_kernel, "exit_latent_kernel": exit_latent_kernel, "stride_offset_vector": stride_offset_vector, "attenuation_speed_exponent": attenuation_speed_exponent, "bypass_coef_vector": bypass_coef_vector, "cluster_rescale_coefs": cluster_rescale_coefs, "blender_result_matrix": blender_result_matrix, "latter_microbatch_activations": latter_microbatch_activations, "specialist_rescale_coefs": specialist_rescale_coefs, "specialist_valve_matrix": specialist_valve_matrix, "specialist_expand_matrix": specialist_expand_matrix, "specialist_contract_matrix": specialist_contract_matrix, "specialist_picks": specialist_picks, "selected_specialist_coefs": selected_specialist_coefs}


NORM_EPS = 1e-06
HIGHEST = lax.Precision.HIGHEST

def conv_silu(inputs, weight):
    tap_count = weight.shape[0]
    context_span = inputs.shape[0]
    padded = jnp.pad(inputs.astype(jnp.float32), ((tap_count - 1, 0), (0, 0)))
    kernel = weight.astype(jnp.float32)
    running_total = kernel[0] * padded[0:context_span]
    for offset in range(1, tap_count):
        running_total = running_total + kernel[offset] * padded[offset:offset + context_span]
    return jax.nn.silu(running_total)

def block_step(carry_state, inputs):
    scaled_x, b_block, c_block, log_block = inputs
    context_span = log_block.shape[0]
    running = jnp.cumsum(log_block, axis=0)
    causal = (jnp.arange(context_span)[:, None] >= jnp.arange(context_span)[None, :])[:, :, None, None]
    log_gap = running[:, None] - running[None, :]
    weights = jnp.where(causal, jnp.exp(jnp.where(causal, log_gap, 0.0)), 0.0)
    scores = jnp.einsum('lgn,sgn->lsg', c_block, b_block, preferred_element_type=jnp.float32)
    inside = jnp.einsum('lsgj,sgjp->lgjp', scores[..., None] * weights, scaled_x, precision=HIGHEST)
    c_wide = c_block.astype(jnp.float32)
    b_wide = b_block.astype(jnp.float32)
    before = jnp.einsum('lgn,gjpn->lgjp', c_wide, carry_state, precision=HIGHEST) * jnp.exp(running)[..., None]
    to_end = jnp.exp(running[-1] - running)
    carry_state = carry_state * jnp.exp(running[-1])[..., None, None] + jnp.einsum('sgn,sgjp->gjpn', b_wide, scaled_x * to_end[..., None], precision=HIGHEST)
    return (carry_state, inside + before)

def rounded_pieces(left, right, pieces):
    block_width = left.shape[1] // pieces
    running_total = jnp.zeros((left.shape[0], right.shape[1]), jnp.float32)
    for piece_index in range(pieces):
        block_term = jnp.dot(left[:, piece_index * block_width:(piece_index + 1) * block_width], right[piece_index * block_width:(piece_index + 1) * block_width], preferred_element_type=jnp.float32).astype(jnp.bfloat16)
        running_total = running_total + lax.optimization_barrier(block_term).astype(jnp.float32)
    return running_total.astype(jnp.bfloat16)

def reference(blender_incoming_features, entry_latent_matrix, exit_latent_matrix, unactivated_valve, presoftplus_strides, extra_attenuation, incoming_feature_kernel, entry_latent_kernel, exit_latent_kernel, stride_offset_vector, attenuation_speed_exponent, bypass_coef_vector, cluster_rescale_coefs, blender_result_matrix, latter_microbatch_activations, specialist_rescale_coefs, specialist_valve_matrix, specialist_expand_matrix, specialist_contract_matrix, specialist_picks, selected_specialist_coefs):
    context_span = blender_incoming_features.shape[0]
    members_within_cluster = HEADS // SHARING_CLUSTERS
    conv_x_out = conv_silu(blender_incoming_features, incoming_feature_kernel).reshape(context_span, SHARING_CLUSTERS, members_within_cluster, HEAD_DIM)
    conv_b_out = conv_silu(entry_latent_matrix, entry_latent_kernel).astype(jnp.bfloat16).reshape(context_span, SHARING_CLUSTERS, STATE)
    conv_c_out = conv_silu(exit_latent_matrix, exit_latent_kernel).astype(jnp.bfloat16).reshape(context_span, SHARING_CLUSTERS, STATE)
    stride_amount = jax.nn.softplus(presoftplus_strides + stride_offset_vector[None, :])
    attenuation_exponent = (-jnp.exp(attenuation_speed_exponent)[None, :] * stride_amount + extra_attenuation).reshape(context_span, SHARING_CLUSTERS, members_within_cluster)
    scaled_x = conv_x_out * stride_amount.reshape(context_span, SHARING_CLUSTERS, members_within_cluster)[..., None]
    blocks = context_span // BLOCK

    def as_blocks(array_value):
        return array_value.reshape((blocks, BLOCK) + array_value.shape[1:])
    start_state = jnp.zeros((SHARING_CLUSTERS, members_within_cluster, HEAD_DIM, STATE), jnp.float32)
    _, block_out = lax.scan(block_step, start_state, (as_blocks(scaled_x), as_blocks(conv_b_out), as_blocks(conv_c_out), as_blocks(attenuation_exponent)))
    ssd_out = block_out.reshape(context_span, SHARING_CLUSTERS, members_within_cluster, HEAD_DIM) + bypass_coef_vector.reshape(SHARING_CLUSTERS, members_within_cluster)[None, :, :, None] * conv_x_out
    gated_out = ssd_out.reshape(context_span, INNER) * jax.nn.silu(unactivated_valve.astype(jnp.float32))
    grouped = gated_out.reshape(context_span, SHARING_CLUSTERS, INNER // SHARING_CLUSTERS)
    grouped = grouped * lax.rsqrt(lax.optimization_barrier(jnp.mean(grouped * grouped, axis=-1, keepdims=True)) + NORM_EPS)
    normed = (grouped.reshape(context_span, INNER) * cluster_rescale_coefs.astype(jnp.float32)).astype(jnp.bfloat16)
    mixed_a = rounded_pieces(normed, blender_result_matrix, N_TP)
    widened = latter_microbatch_activations.astype(jnp.float32)
    normed_b = (widened * lax.rsqrt(lax.optimization_barrier(jnp.mean(widened * widened, axis=-1, keepdims=True)) + NORM_EPS) * specialist_rescale_coefs.astype(jnp.float32)).astype(jnp.bfloat16)
    flat_routes = specialist_picks.reshape(-1).astype(jnp.int32)
    assigned = flat_routes.shape[0]
    sorted_order = jnp.argsort(flat_routes, stable=True).astype(jnp.int32)
    routes_sorted = flat_routes[sorted_order]
    tokens_sorted = (sorted_order // TOPK).astype(jnp.int32)
    counts = lax.optimization_barrier(jnp.sum((flat_routes[:, None] == jnp.arange(EXPERTS, dtype=jnp.int32)[None, :]).astype(jnp.int32), axis=0)).astype(jnp.int32)
    starts = (jnp.cumsum(counts) - counts).astype(jnp.int32)
    place_sorted = (jnp.arange(assigned, dtype=jnp.int32) - starts[routes_sorted]).astype(jnp.int32)
    places = jnp.zeros((assigned,), jnp.int32).at[sorted_order].set(place_sorted)
    capacity_all = N_EP * CAP

    def one_expert(expert):
        slots = jnp.arange(capacity_all, dtype=jnp.int32)
        is_valid = slots < counts[expert]
        token_ids = tokens_sorted[jnp.minimum(starts[expert] + slots, assigned - 1)]
        chosen = jnp.where(is_valid[:, None], normed_b[token_ids], jnp.zeros((), jnp.bfloat16))
        gate_sum = jnp.dot(chosen, specialist_valve_matrix[expert], preferred_element_type=jnp.float32)
        up_sum = jnp.dot(chosen, specialist_expand_matrix[expert], preferred_element_type=jnp.float32)
        hidden = (jax.nn.silu(gate_sum) * up_sum).astype(jnp.bfloat16)
        return rounded_pieces(hidden, specialist_contract_matrix[expert], N_TP)
    results = lax.map(one_expert, jnp.arange(EXPERTS, dtype=jnp.int32))
    picked = results[flat_routes, places].astype(jnp.float32) * selected_specialist_coefs.reshape(assigned, 1)
    mixed_b = lax.optimization_barrier(jnp.sum(picked.reshape(assigned // TOPK, TOPK, D), axis=1)).astype(jnp.bfloat16)
    return (mixed_a, mixed_b)
```

```python
import functools

import jax
import jax.numpy as jnp
from jax import lax
from jax.experimental import pallas as pl
from jax.experimental.pallas import tpu as pltpu
from jax.sharding import PartitionSpec as P

HEADS = 64
HEAD_DIM = 64
SHARING_CLUSTERS = 16
STATE = 128
TOPK = 2

NORM_EPS = 1e-06
HIGHEST = lax.Precision.HIGHEST
MESH = pl.DeviceIdType.MESH
F32 = jnp.float32
BF16 = jnp.bfloat16
HALO = 16
LANES = 128
CHUNKS = 4


def silu(v):
    return v / (1.0 + jnp.exp(-v))


def dot(a, b):
    return jnp.dot(a, b, preferred_element_type=F32)


def dot_last(a, b, precision=None):
    return lax.dot_general(
        a, b, (((1,), (1,)), ((), ())), preferred_element_type=F32, precision=precision
    )


def widen(per_head, first, count, rows):
    lane = lax.broadcasted_iota(jnp.int32, (rows, LANES), 1)
    pieces = []
    for h in range(first, first + count, 2):
        left = jnp.broadcast_to(per_head[:, h : h + 1], (rows, LANES))
        right = jnp.broadcast_to(per_head[:, h + 1 : h + 2], (rows, LANES))
        pieces.append(jnp.where(lane < HEAD_DIM, left, right))
    return jnp.concatenate(pieces, axis=1)


def layer_kernel(
    E,
    T,
    picks_h,
    coefs_h,
    act_h,
    bgain_h,
    x_h,
    b_h,
    c_h,
    kx_h,
    kb_h,
    kc_h,
    pre_h,
    extra_h,
    valve_h,
    again_h,
    wg_h,
    wu_h,
    wd_h,
    wr_h,
    offset_s,
    speed_s,
    bypass_s,
    outa_ref,
    outb_ref,
    picks_v,
    coefs_v,
    act_v,
    bgain_v,
    x_v,
    b_v,
    c_v,
    kx_v,
    kb_v,
    kc_v,
    pre_v,
    extra_v,
    valve_v,
    again_v,
    wg_v,
    wu_v,
    wd_v,
    wr_v,
    nb,
    out,
    X,
    hid,
    tc,
    fc,
    own,
    ys,
    yr,
    fin,
    ret,
    acc,
    cols_v,
    rim,
    joined,
    ybuf,
    cc_v,
    grown_v,
    state,
    st16,
    peerst,
    dec_v,
    peerdec,
    chin,
    chout,
    enter,
    esend,
    normed,
    atc,
    afc,
    aown,
    ays,
    ayr,
    load_sem,
    a2a_s,
    a2a_r,
    yg_s,
    yg_r,
    cg_s,
    cg_r,
    rc_s,
    rc_r,
    ry_s,
    ry_r,
    rt_s,
    rt_r,
    mc_s,
    mc_r,
    my_s,
    my_r,
    rim_s,
    rim_r,
    st_s,
    st_r,
):
    e = lax.axis_index("ep")
    t = lax.axis_index("tp")
    y = lax.div(t, 2)
    c = lax.rem(t, 2)
    NY = T // 2
    bpc = E // CHUNKS
    tok, width = act_v.shape
    S = width // T
    C = out.shape[1]
    M = bpc * C
    rows, channels = x_v.shape
    latent = b_v.shape[1]
    heads = pre_v.shape[0]
    groups = latent // STATE
    members = heads // groups
    wide = members * HEAD_DIM
    taps = kx_v.shape[0]
    half = STATE // 2
    U = wg_v.shape[1]

    pairs = [
        (picks_h, picks_v),
        (coefs_h, coefs_v),
        (act_h, act_v),
        (bgain_h, bgain_v),
        (x_h, x_v),
        (b_h, b_v),
        (c_h, c_v),
        (kx_h, kx_v),
        (kb_h, kb_v),
        (kc_h, kc_v),
        (pre_h, pre_v),
        (extra_h, extra_v),
        (wg_h, wg_v),
        (wu_h, wu_v),
        (wd_h, wd_v),
        (valve_h, valve_v),
        (again_h, again_v),
        (wr_h, wr_v),
    ]
    loads = {}
    for i, (src, dst) in enumerate(pairs):
        loads[i] = pltpu.make_async_copy(src, dst, load_sem.at[i])
        loads[i].start()

    def ep_peer(j):
        return (jnp.bitwise_xor(e, j), t)

    def y_peer(m):
        return (e, jnp.bitwise_xor(y, m) * 2 + c)

    core_peer = (e, y * 2 + 1 - c)

    barrier = pltpu.get_barrier_semaphore()
    peers = [ep_peer(j) for j in range(1, E)] + [y_peer(m) for m in range(1, NY)] + [core_peer]
    for peer in peers:
        pl.semaphore_signal(barrier, inc=1, device_id=peer, device_id_type=MESH)

    sends = []

    def rcopy(src, dst, ssem, rsem, dev):
        return pltpu.make_async_remote_copy(
            src_ref=src,
            dst_ref=dst,
            send_sem=ssem,
            recv_sem=rsem,
            device_id=dev,
            device_id_type=MESH,
        )

    def send(*args):
        copy = rcopy(*args)
        copy.start()
        sends.append(copy)

    def arrive(dst, rsem):
        rcopy(dst, dst, a2a_s.at[0], rsem, core_peer).wait_recv()

    for i in range(4):
        loads[i].wait()
    pick = jnp.bitwise_xor(picks_v[...], e)
    expert = lax.broadcasted_iota(jnp.int32, (E, tok), 0)
    row_i = lax.broadcasted_iota(jnp.int32, (tok, tok), 0)
    col_i = lax.broadcasted_iota(jnp.int32, (tok, tok), 1)
    before = (row_i < col_i).astype(BF16)
    hot0 = (expert == pick[0:1]).astype(F32)
    hot1 = (expert == pick[1:2]).astype(F32)
    cum0 = dot(hot0.astype(BF16), before)
    cum1 = dot(hot1.astype(BF16), before) + jnp.sum(hot0, axis=1, keepdims=True)
    rank0 = jnp.sum(hot0 * cum0, axis=0, keepdims=True)
    rank1 = jnp.sum(hot1 * cum1, axis=0, keepdims=True)
    slot0 = pick[0:1].astype(F32) * float(C) + rank0
    slot1 = pick[1:2].astype(F32) * float(C) + rank1
    stacked = jnp.concatenate(
        [slot0, slot1, coefs_v[...], jnp.zeros((4, tok), F32)], axis=0
    )
    cols_v[...] = stacked.T

    wide_act = act_v[...].astype(F32)
    scale = lax.rsqrt(jnp.mean(wide_act * wide_act, axis=1, keepdims=True) + NORM_EPS)
    nb[...] = (wide_act * scale * bgain_v[...].astype(F32)).astype(BF16)

    def placing(j):
        slot = (lax.broadcasted_iota(jnp.int32, (C, tok), 0) + j * C).astype(F32)
        return ((slot == slot0) | (slot == slot1)).astype(BF16)

    mine = nb[:, pl.ds(pl.multiple_of(t * S, S), S)]
    for j in range(1, E):
        out[j] = dot(placing(j), mine).astype(BF16)
        if j == 1:
            pl.semaphore_wait(barrier, len(peers))
        send(out.at[j], X.at[t, j], a2a_s.at[j], a2a_r.at[j // bpc], ep_peer(j))

    for i in range(4, 12):
        loads[i].wait()
    tail = pl.ds(rows - HALO, HALO)
    rims = [
        (x_v.at[tail], rim.at[:, pl.ds(0, channels)]),
        (b_v.at[tail], rim.at[:, pl.ds(channels, latent)]),
        (c_v.at[tail], rim.at[:, pl.ds(channels + latent, latent)]),
    ]
    following = (jnp.minimum(e + 1, E - 1), t)

    def rim_copy(i):
        return rcopy(rims[i][0], rims[i][1], rim_s.at[i], rim_r.at[i], following)

    @pl.when(e < E - 1)
    def _():
        for i in range(3):
            rim_copy(i).start()

    @pl.when(e == 0)
    def _():
        rim[...] = jnp.zeros(rim.shape, BF16)

    first = placing(0)
    for tt in range(T):
        X[tt, 0] = dot(first, nb[:, tt * S : (tt + 1) * S]).astype(BF16)

    def span(k):
        return pl.ds(1, bpc - 1) if k == 0 else pl.ds(k * bpc, bpc)

    def share(m, cc):
        return jnp.bitwise_xor(y, m) * 2 + cc

    def forward(k):
        if k == 0 and bpc == 1:
            return
        block = X.at[t, span(k)]
        arrive(block, a2a_r.at[k])
        for m in range(1, NY):
            send(block, block, yg_s.at[m, k], yg_r.at[m, k], y_peer(m))
        send(block, block, cg_s.at[0, k], cg_r.at[0, k], core_peer)

    def forward_core(k):
        if k == 0 and bpc == 1:
            return
        for m in range(1, NY):
            block = X.at[share(m, c), span(k)]
            arrive(block, yg_r.at[m, k])
            send(block, block, cg_s.at[m, k], cg_r.at[m, k], core_peer)

    def ready(k):
        if k == 0 and bpc == 1:
            return
        for m in range(NY):
            arrive(X.at[share(m, 1 - c), span(k)], cg_r.at[m, k])

    NT = min(256, U)
    NS = min(256, S)

    def gate_up(k):
        def body(n, carry):
            at = pl.ds(pl.multiple_of(n * NT, NT), NT)
            gate = up = None
            for tt in range(T):
                r = X[tt, k * bpc : (k + 1) * bpc].reshape(M, S)
                deep = slice(tt * S, (tt + 1) * S)
                g = dot(r, wg_v[deep, at])
                u = dot(r, wu_v[deep, at])
                gate = g if gate is None else gate + g
                up = u if up is None else up + u
            hid[:, at] = (silu(gate) * up).astype(BF16)
            return carry

        lax.fori_loop(0, U // NT, body, 0)

    def down(k):
        for core in (1 - c, c):
            for m in list(range(1, NY)) + [0]:
                base = share(m, core) * S
                for n in range(S // NS):
                    at = pl.ds(pl.multiple_of(base + n * NS, NS), NS)
                    part = dot(hid[...], wd_v[:, at])
                    if core is c:
                        own[k, m, :, n * NS : (n + 1) * NS] = part
                    else:
                        tc[k, m, :, n * NS : (n + 1) * NS] = part.astype(BF16)
                if core is not c:
                    send(tc.at[k, m], fc.at[k, m], rc_s.at[m, k], rc_r.at[m, k], core_peer)

    def reduce_core(k):
        for m in list(range(1, NY)) + [0]:
            arrive(fc.at[k, m], rc_r.at[m, k])
            total = own[k, m] + fc[k, m].astype(F32)
            if m == 0:
                own[k, 0] = total
            else:
                ys[k, m] = total.astype(BF16)
                send(ys.at[k, m], yr.at[k, m], ry_s.at[m, k], ry_r.at[m, k], y_peer(m))

    def reduce_y(k):
        total = own[k, 0]
        for m in range(1, NY):
            arrive(yr.at[k, m], ry_r.at[m, k])
            total = total + yr[k, m].astype(F32)
        done = total.astype(BF16).reshape(bpc, C, S)
        for i in range(bpc):
            j = k * bpc + i
            if j == 0:
                ret[0] = done[0]
            else:
                fin[j] = done[i]
                send(fin.at[j], ret.at[j], rt_s.at[j], rt_r.at[k], ep_peer(j))

    def combine(k):
        if not (k == 0 and bpc == 1):
            arrive(ret.at[span(k)], rt_r.at[k])
        block = ret[k * bpc : (k + 1) * bpc].reshape(M, S)
        lane = (lax.broadcasted_iota(jnp.int32, (tok, M), 1) + k * M).astype(F32)
        total = None
        for p in range(TOPK):
            chosen = (lane == cols_v[:, p : p + 1]).astype(BF16)
            term = dot(chosen, block) * cols_v[:, TOPK + p : TOPK + p + 1]
            total = term if total is None else total + term
        if k > 0:
            total = total + acc[...]
        if k < CHUNKS - 1:
            acc[...] = total
        else:
            outb_ref[...] = total.astype(BF16)

    causal = row_i >= col_i

    def conv(ref, k_ref, start, size, rim_start):
        joined[0:HALO, 0:size] = rim[:, rim_start : rim_start + size].astype(F32)
        joined[HALO : HALO + rows, 0:size] = ref[:, start : start + size].astype(F32)
        kernel = k_ref[:, start : start + size].astype(F32)
        total = None
        for j in range(taps):
            at = HALO - taps + 1 + j
            term = kernel[j : j + 1] * joined[at : at + rows, 0:size]
            total = term if total is None else total + term
        return silu(total)

    def column(ref):
        index = lax.broadcasted_iota(jnp.int32, (heads, rows), 0)
        value = jnp.zeros((heads, rows), F32)
        for h in range(heads):
            value = jnp.where(index == h, ref[h], value)
        return value

    z = pre_v[...] + column(offset_s)
    step_t = jnp.maximum(z, 0.0) + jnp.log1p(jnp.exp(-jnp.abs(z)))
    decay_t = -jnp.exp(column(speed_s)) * step_t + extra_v[...]
    tri = causal.astype(F32)
    eye = (row_i == col_i).astype(F32)
    run = dot_last(tri, decay_t, HIGHEST)
    run_t = dot_last(decay_t, tri, HIGHEST)
    step = dot_last(eye, step_t, HIGHEST)
    last = run[rows - 1 : rows]
    to_end = jnp.exp(last - run)
    grown_v[...] = jnp.exp(run)
    lane128 = lax.broadcasted_iota(jnp.int32, (rows, LANES), 1)
    dec_row = widen(jnp.exp(last), 0, heads, 1)
    dec_v[...] = jnp.broadcast_to(dec_row, dec_v.shape)

    def ssd(g):
        lead = g * members
        cols = slice(g * wide, (g + 1) * wide)
        xc = conv(x_v, kx_v, g * wide, wide, g * wide)
        bb = conv(b_v, kb_v, g * STATE, STATE, channels + g * STATE).astype(BF16)
        cc = conv(c_v, kc_v, g * STATE, STATE, channels + latent + g * STATE).astype(BF16)
        cc_v[:, g * STATE : (g + 1) * STATE] = cc
        xs = xc * widen(step, lead, members, rows)
        xs16 = xs.astype(BF16)
        scores = dot_last(cc, bb)
        scores = jnp.where(causal, scores, 0.0)
        inside = []
        skip = []
        for pair in range(0, members, 2):
            x_pair = xs16[:, pair * HEAD_DIM : (pair + 2) * HEAD_DIM]
            both = []
            for h in (lead + pair, lead + pair + 1):
                gap = jnp.minimum(run[:, h : h + 1] - run_t[h : h + 1, :], 0.0)
                weights = (jnp.exp(gap) * scores).astype(BF16)
                both.append(dot(weights, x_pair))
            inside.append(jnp.where(lane128 < HEAD_DIM, both[0], both[1]))
            h = lead + pair
            skip.append(jnp.where(lane128 < HEAD_DIM, bypass_s[h], bypass_s[h + 1]))
        ybuf[:, cols] = jnp.concatenate(inside, axis=1) + xc * jnp.concatenate(skip, axis=1)
        x_end = (xs * widen(to_end, lead, members, rows)).astype(BF16)
        state[:, cols] = lax.dot_general(
            bb, x_end, (((0,), (0,)), ((), ())), preferred_element_type=F32
        )

    side = lax.rem(e, 2)
    group = lax.div(e, 2)
    pairs_count = E // 2

    def state_exchange():
        st16[0] = state[0:half].astype(BF16)
        st16[1] = state[half:STATE].astype(BF16)
        send(st16.at[1 - side], peerst, st_s.at[0], st_r.at[0], ep_peer(1))
        send(dec_v, peerdec, st_s.at[1], st_r.at[1], ep_peer(1))

    behind = (jnp.maximum(e - 2, 0), t)
    ahead = (jnp.minimum(e + 2, E - 1), t)

    def chain(low, high):
        @pl.when((group >= low) & (group < high))
        def _():
            arrive(peerst, st_r.at[0])
            arrive(peerdec, st_r.at[1])
            own_half = st16[side].astype(F32)
            other = peerst[...].astype(F32)
            own_dec = dec_v[0:1]
            other_dec = peerdec[0:1]
            left = side == 0
            s0 = jnp.where(left, own_half, other)
            s1 = jnp.where(left, other, own_half)
            d0 = jnp.where(left, own_dec, other_dec)
            d1 = jnp.where(left, other_dec, own_dec)

            @pl.when(group > 0)
            def _():
                arrive(chin, st_r.at[2])

            @pl.when(group == 0)
            def _():
                chin[...] = jnp.zeros(chin.shape, BF16)

            e0 = chin[...].astype(F32)
            e1 = e0 * d0 + s0

            @pl.when(group < pairs_count - 1)
            def _():
                chout[...] = (e1 * d1 + s1).astype(BF16)
                rcopy(chout, chin, st_s.at[2], st_r.at[2], ahead).start()

            enter[side] = jnp.where(left, e0, e1).astype(BF16)
            esend[...] = jnp.where(left, e1, e0).astype(BF16)
            rcopy(esend, enter.at[side], st_s.at[3], st_r.at[3], ep_peer(1)).start()

    def gate_norm():
        arrive(enter.at[1 - side], st_r.at[3])
        entered = enter[...].reshape(STATE, channels)
        for g in range(groups):
            cols = slice(g * wide, (g + 1) * wide)
            carried = dot(cc_v[:, g * STATE : (g + 1) * STATE], entered[:, cols])
            ssd_out = ybuf[:, cols] + carried * widen(grown_v[...], g * members, members, rows)
            gated = ssd_out * silu(valve_v[:, cols].astype(F32))
            norm = lax.rsqrt(jnp.mean(gated * gated, axis=1, keepdims=True) + NORM_EPS)
            normed[:, cols] = (gated * norm * again_v[:, cols].astype(F32)).astype(BF16)

    width_a = wr_v.shape[1]
    NA = min(512, width_a)
    R = rows // T

    def project():
        for n in range(width_a // NA):
            part = dot(normed[...], wr_v[:, n * NA : (n + 1) * NA])
            for yy in range(NY):
                m = jnp.bitwise_xor(y, yy)
                low = part[(yy * 2) * R : (yy * 2 + 1) * R]
                high = part[(yy * 2 + 1) * R : (yy * 2 + 2) * R]
                aown[m, :, n * NA : (n + 1) * NA] = jnp.where(c == 0, low, high)
                atc[m, :, n * NA : (n + 1) * NA] = jnp.where(c == 0, high, low).astype(BF16)
        for m in list(range(1, NY)) + [0]:
            send(atc.at[m], afc.at[m], mc_s.at[m], mc_r.at[m], core_peer)

    def mix_core():
        for m in list(range(1, NY)) + [0]:
            arrive(afc.at[m], mc_r.at[m])
            total = aown[m] + afc[m].astype(F32)
            if m == 0:
                aown[0] = total
            else:
                ays[m] = total.astype(BF16)
                send(ays.at[m], ayr.at[m], my_s.at[m], my_r.at[m], y_peer(m))

    def mix_y():
        total = aown[0]
        for m in range(1, NY):
            arrive(ayr.at[m], my_r.at[m])
            total = total + ayr[m].astype(F32)
        outa_ref[...] = total.astype(BF16)

    @pl.when(e > 0)
    def _():
        for i in range(3):
            arrive(rims[i][1], rim_r.at[i])

    for g in range(groups):
        ssd(g)
        if g == 0:
            forward(0)
        if g == 1:
            forward_core(0)
            forward(1)
    if groups < 2:
        forward_core(0)
        forward(1)
    state_exchange()
    ready(0)
    for i in (12, 13, 14):
        loads[i].wait()
    bounds = [round(i * pairs_count / 4) for i in range(5)]
    gate_up(0)
    forward_core(1)
    forward(2)
    chain(bounds[0], bounds[1])
    down(0)
    ready(1)
    gate_up(1)
    chain(bounds[1], bounds[2])
    reduce_core(0)
    forward_core(2)
    forward(3)
    down(1)
    reduce_y(0)
    chain(bounds[2], bounds[3])
    ready(2)
    gate_up(2)
    reduce_core(1)
    forward_core(3)
    down(2)
    chain(bounds[3], bounds[4])
    reduce_y(1)
    combine(0)
    ready(3)
    gate_up(3)
    reduce_core(2)
    down(3)
    for i in (15, 16, 17):
        loads[i].wait()
    gate_norm()
    reduce_y(2)
    reduce_core(3)
    project()
    combine(1)
    mix_core()
    reduce_y(3)
    combine(2)
    mix_y()
    combine(3)

    for copy in sends:
        copy.wait_send()

    @pl.when(e < E - 1)
    def _():
        for i in range(3):
            rim_copy(i).wait_send()

    @pl.when(group < pairs_count - 1)
    def _():
        rcopy(chout, chin, st_s.at[2], st_r.at[2], ahead).wait_send()

    rcopy(esend, enter.at[side], st_s.at[3], st_r.at[3], ep_peer(1)).wait_send()


def local(
    blender_incoming_features,
    entry_latent_matrix,
    exit_latent_matrix,
    unactivated_valve,
    presoftplus_strides,
    extra_attenuation,
    incoming_feature_kernel,
    entry_latent_kernel,
    exit_latent_kernel,
    stride_offset_vector,
    attenuation_speed_exponent,
    bypass_coef_vector,
    cluster_rescale_coefs,
    blender_result_matrix,
    latter_microbatch_activations,
    specialist_rescale_coefs,
    specialist_valve_matrix,
    specialist_expand_matrix,
    specialist_contract_matrix,
    specialist_picks,
    selected_specialist_coefs,
):
    E = lax.axis_size("ep")
    T = lax.axis_size("tp")
    NY = T // 2
    rows, channels = blender_incoming_features.shape
    latent = entry_latent_matrix.shape[1]
    heads = presoftplus_strides.shape[1]
    taps = incoming_feature_kernel.shape[0]
    wide = channels // (latent // STATE)
    half = STATE // 2
    tok, width = latter_microbatch_activations.shape
    S = width // T
    C = 3 * tok * TOPK // (2 * E)
    bpc = E // CHUNKS
    M = bpc * C
    wg, wu, wd = specialist_valve_matrix[0], specialist_expand_matrix[0], specialist_contract_matrix[0]
    U = wg.shape[1]
    width_a = blender_result_matrix.shape[1]
    R = rows // T
    far = [
        specialist_picks.T,
        selected_specialist_coefs.T,
        latter_microbatch_activations,
        specialist_rescale_coefs[None, :],
        blender_incoming_features,
        entry_latent_matrix,
        exit_latent_matrix,
        incoming_feature_kernel,
        entry_latent_kernel,
        exit_latent_kernel,
        presoftplus_strides.T,
        extra_attenuation.T,
        unactivated_valve,
        cluster_rescale_coefs[None, :],
        wg,
        wu,
        wd,
        blender_result_matrix,
    ]
    near = [stride_offset_vector, attenuation_speed_exponent, bypass_coef_vector]
    landing = [pltpu.VMEM(a.shape, a.dtype) for a in far]
    dma = pltpu.SemaphoreType.DMA
    vmem = pltpu.VMEM
    return pl.pallas_call(
        functools.partial(layer_kernel, E, T),
        in_specs=[pl.BlockSpec(memory_space=pl.ANY)] * len(far)
        + [pl.BlockSpec(memory_space=pltpu.SMEM)] * len(near),
        out_specs=[pl.BlockSpec(memory_space=pltpu.VMEM)] * 2,
        out_shape=[
            jax.ShapeDtypeStruct((R, width_a), BF16),
            jax.ShapeDtypeStruct((tok, S), BF16),
        ],
        scratch_shapes=landing
        + [
            vmem((tok, width), BF16),
            vmem((E, C, S), BF16),
            vmem((T, E, C, S), BF16),
            vmem((M, U), BF16),
            vmem((CHUNKS, NY, M, S), BF16),
            vmem((CHUNKS, NY, M, S), BF16),
            vmem((CHUNKS, NY, M, S), F32),
            vmem((CHUNKS, NY, M, S), BF16),
            vmem((CHUNKS, NY, M, S), BF16),
            vmem((E, C, S), BF16),
            vmem((E, C, S), BF16),
            vmem((tok, S), F32),
            vmem((tok, 8), F32),
            vmem((HALO, channels + 2 * latent), BF16),
            vmem((rows + HALO, wide), F32),
            vmem((rows, channels), F32),
            vmem((rows, latent), BF16),
            vmem((rows, heads), F32),
            vmem((STATE, channels), F32),
            vmem((2, half, channels), BF16),
            vmem((half, channels), BF16),
            vmem((8, channels), F32),
            vmem((8, channels), F32),
            vmem((half, channels), BF16),
            vmem((half, channels), BF16),
            vmem((2, half, channels), BF16),
            vmem((half, channels), BF16),
            vmem((rows, channels), BF16),
            vmem((NY, R, width_a), BF16),
            vmem((NY, R, width_a), BF16),
            vmem((NY, R, width_a), F32),
            vmem((NY, R, width_a), BF16),
            vmem((NY, R, width_a), BF16),
            dma((len(far),)),
            dma((E,)),
            dma((CHUNKS,)),
            dma((NY, CHUNKS)),
            dma((NY, CHUNKS)),
            dma((NY, CHUNKS)),
            dma((NY, CHUNKS)),
            dma((NY, CHUNKS)),
            dma((NY, CHUNKS)),
            dma((NY, CHUNKS)),
            dma((NY, CHUNKS)),
            dma((E,)),
            dma((CHUNKS,)),
            dma((NY,)),
            dma((NY,)),
            dma((NY,)),
            dma((NY,)),
            dma((3,)),
            dma((3,)),
            dma((4,)),
            dma((4,)),
        ],
        compiler_params=pltpu.CompilerParams(
            collective_id=0, has_side_effects=True, vmem_limit_bytes=60 * 1024 * 1024
        ),
        name="layer",
    )(*far, *near)


def solution(mesh):
    in_specs = (
        P("ep", "tp"),
        P("ep", "tp"),
        P("ep", "tp"),
        P("ep", "tp"),
        P("ep", "tp"),
        P("ep", "tp"),
        P(None, "tp"),
        P(None, "tp"),
        P(None, "tp"),
        P("tp"),
        P("tp"),
        P("tp"),
        P("tp"),
        P("tp", None),
        P("ep", None),
        P(),
        P("ep", None, "tp"),
        P("ep", None, "tp"),
        P("ep", "tp", None),
        P("ep", None),
        P("ep", None),
    )
    out_specs = (P(("ep", "tp"), None), P("ep", "tp"))
    return jax.shard_map(local, mesh=mesh, in_specs=in_specs, out_specs=out_specs, check_vma=False)
```

```python
import functools

import jax
import jax.numpy as jnp
from jax import lax
from jax.experimental import pallas as pl
from jax.experimental.pallas import tpu as pltpu
from jax.sharding import PartitionSpec as P

HEADS = 64
HEAD_DIM = 64
SHARING_CLUSTERS = 16
STATE = 128
TOPK = 2

NORM_EPS = 1e-06
HIGHEST = lax.Precision.HIGHEST
MESH = pl.DeviceIdType.MESH
F32 = jnp.float32
BF16 = jnp.bfloat16
HALO = 16
LANES = 128
UNITS = 8
GROUPS = ((0, 1), (1, 1), (2, 2), (4, 2), (6, 2))
SENDING = (2, 3, 5, 1, 4, 6, 7)

ORDER = (
    ("mp",),
    ("fw", 0),
    ("ssd", 0),
    ("ssd", 1),
    ("fw", 2),
    ("ssd", 2),
    ("ssd", 3),
    ("rd", 0),
    ("sx",),
    ("fc", 0),
    ("fw", 4),
    ("lw",),
    ("gu", 0),
    ("dn", 0),
    ("ch", 0),
    ("fc", 2),
    ("fc", 1),
    ("fc", 4),
    ("fw", 6),
    ("rd", 4),
    ("ch", 1),
    ("fw", 1),
    ("gu", 4),
    ("rd", 2),
    ("dn", 4),
    ("fc", 6),
    ("rd", 1),
    ("rc", 4),
    ("rd", 6),
    ("ch", 2),
    ("gu", 6),
    ("dn", 6),
    ("rc", 0),
    ("ry", 4),
    ("gu", 1),
    ("rc", 6),
    ("ch", 3),
    ("dn", 1),
    ("gu", 2),
    ("dn", 2),
    ("rc", 1),
    ("ry", 6),
    ("lr",),
    ("gn",),
    ("rc", 2),
    ("pj",),
    ("ry", 1),
    ("mc",),
    ("ry", 2),
    ("cb", 4),
    ("ry", 0),
    ("cb", 1),
    ("cb", 6),
    ("cb", 0),
    ("cb", 2),
    ("my",),
)


def silu(v):
    return v / (1.0 + jnp.exp(-v))


def dot(a, b):
    return jnp.dot(a, b, preferred_element_type=F32)


def dot_last(a, b, precision=None):
    return lax.dot_general(
        a, b, (((1,), (1,)), ((), ())), preferred_element_type=F32, precision=precision
    )


def widen(per_head, first, count, rows):
    lane = lax.broadcasted_iota(jnp.int32, (rows, LANES), 1)
    pieces = []
    for h in range(first, first + count, 2):
        left = jnp.broadcast_to(per_head[:, h : h + 1], (rows, LANES))
        right = jnp.broadcast_to(per_head[:, h + 1 : h + 2], (rows, LANES))
        pieces.append(jnp.where(lane < HEAD_DIM, left, right))
    return jnp.concatenate(pieces, axis=1)


def layer_kernel(
    E,
    T,
    picks_h,
    coefs_h,
    act_h,
    bgain_h,
    x_h,
    b_h,
    c_h,
    kx_h,
    kb_h,
    kc_h,
    pre_h,
    extra_h,
    valve_h,
    again_h,
    wg_h,
    wu_h,
    wd_h,
    wr_h,
    offset_s,
    speed_s,
    bypass_s,
    outa_ref,
    outb_ref,
    picks_v,
    coefs_v,
    act_v,
    bgain_v,
    x_v,
    b_v,
    c_v,
    kx_v,
    kb_v,
    kc_v,
    pre_v,
    extra_v,
    valve_v,
    again_v,
    wg_v,
    wu_v,
    wd_v,
    wr_v,
    nb,
    out,
    out1,
    X,
    hid,
    tc,
    fc,
    own,
    ys,
    yr,
    fin,
    ret,
    acc,
    cols_v,
    rim,
    joined,
    ybuf,
    cc_v,
    grown_v,
    state,
    st16,
    peerst,
    dec_v,
    peerdec,
    chin,
    chout,
    enter,
    esend,
    normed,
    atc,
    afc,
    aown,
    ays,
    ayr,
    load_sem,
    a2a_s,
    a2a_r,
    a2a_r1,
    yg_s,
    yg_r,
    cg_s,
    cg_r,
    rc_s,
    rc_r,
    ry_s,
    ry_r,
    rt_s,
    rt_r,
    mc_s,
    mc_r,
    my_s,
    my_r,
    rim_s,
    rim_r,
    st_s,
    st_r,
):
    e = lax.axis_index("ep")
    t = lax.axis_index("tp")
    y = lax.div(t, 2)
    c = lax.rem(t, 2)
    NY = T // 2
    b = E // UNITS
    blocks = {first: (first * b, count * b) for first, count in GROUPS}
    chunk_of = {}
    for k, (j0, n) in blocks.items():
        for j in range(j0, j0 + n):
            chunk_of[j] = k
    tok, width = act_v.shape
    S = width // T
    C = out.shape[1]
    rows, channels = x_v.shape
    latent = b_v.shape[1]
    heads = pre_v.shape[0]
    groups = latent // STATE
    members = heads // groups
    wide = members * HEAD_DIM
    taps = kx_v.shape[0]
    half = STATE // 2
    U = wg_v.shape[1]

    pairs = [
        (picks_h, picks_v),
        (coefs_h, coefs_v),
        (act_h, act_v),
        (bgain_h, bgain_v),
        (x_h, x_v),
        (b_h, b_v),
        (c_h, c_v),
        (kx_h, kx_v),
        (kb_h, kb_v),
        (kc_h, kc_v),
        (pre_h, pre_v),
        (extra_h, extra_v),
        (wg_h, wg_v),
        (wu_h, wu_v),
        (wd_h, wd_v),
        (valve_h, valve_v),
        (again_h, again_v),
        (wr_h, wr_v),
    ]
    loads = {}
    for i, (src, dst) in enumerate(pairs):
        loads[i] = pltpu.make_async_copy(src, dst, load_sem.at[i])
        loads[i].start()

    def ep_peer(j):
        return (jnp.bitwise_xor(e, j), t)

    def y_peer(m):
        return (e, jnp.bitwise_xor(y, m) * 2 + c)

    core_peer = (e, y * 2 + 1 - c)

    barrier = pltpu.get_barrier_semaphore()
    peers = [ep_peer(j) for j in range(1, E)] + [y_peer(m) for m in range(1, NY)] + [core_peer]
    for peer in peers:
        pl.semaphore_signal(barrier, inc=1, device_id=peer, device_id_type=MESH)

    sends = []

    def rcopy(src, dst, ssem, rsem, dev):
        return pltpu.make_async_remote_copy(
            src_ref=src,
            dst_ref=dst,
            send_sem=ssem,
            recv_sem=rsem,
            device_id=dev,
            device_id_type=MESH,
        )

    def send(*args):
        copy = rcopy(*args)
        copy.start()
        sends.append(copy)

    def arrive(dst, rsem):
        rcopy(dst, dst, a2a_s.at[0, 0], rsem, core_peer).wait_recv()

    with jax.named_scope("load_b"):
        for i in range(4):
            loads[i].wait()
    pick = jnp.bitwise_xor(picks_v[...], e)
    expert = lax.broadcasted_iota(jnp.int32, (E, tok), 0)
    row_i = lax.broadcasted_iota(jnp.int32, (tok, tok), 0)
    col_i = lax.broadcasted_iota(jnp.int32, (tok, tok), 1)
    before = (row_i < col_i).astype(BF16)
    hot0 = (expert == pick[0:1]).astype(F32)
    hot1 = (expert == pick[1:2]).astype(F32)
    cum0 = dot(hot0.astype(BF16), before)
    cum1 = dot(hot1.astype(BF16), before) + jnp.sum(hot0, axis=1, keepdims=True)
    rank0 = jnp.sum(hot0 * cum0, axis=0, keepdims=True)
    rank1 = jnp.sum(hot1 * cum1, axis=0, keepdims=True)
    slot0 = pick[0:1].astype(F32) * float(C) + rank0
    slot1 = pick[1:2].astype(F32) * float(C) + rank1
    stacked = jnp.concatenate(
        [slot0, slot1, coefs_v[...], jnp.zeros((4, tok), F32)], axis=0
    )
    cols_v[...] = stacked.T

    wide_act = act_v[...].astype(F32)
    scale = lax.rsqrt(jnp.mean(wide_act * wide_act, axis=1, keepdims=True) + NORM_EPS)
    nb[...] = (wide_act * scale * bgain_v[...].astype(F32)[None, :]).astype(BF16)

    def placing(j):
        slot = (lax.broadcasted_iota(jnp.int32, (C, tok), 0) + j * C).astype(F32)
        return ((slot == slot0) | (slot == slot1)).astype(BF16)

    with jax.named_scope("load_a"):
        for i in range(4, 12):
            loads[i].wait()
    with jax.named_scope("barrier"):
        pl.semaphore_wait(barrier, len(peers))
    tail = pl.ds(rows - HALO, HALO)
    rims = [
        (x_v.at[tail], rim.at[:, pl.ds(0, channels)]),
        (b_v.at[tail], rim.at[:, pl.ds(channels, latent)]),
        (c_v.at[tail], rim.at[:, pl.ds(channels + latent, latent)]),
    ]
    following = (jnp.minimum(e + 1, E - 1), t)

    def rim_copy(i):
        return rcopy(rims[i][0], rims[i][1], rim_s.at[i], rim_r.at[i], following)

    @pl.when(e < E - 1)
    def _():
        for i in range(3):
            rim_copy(i).start()

    @pl.when(e == 0)
    def _():
        rim[...] = jnp.zeros(rim.shape, BF16)

    def normed_share(tt):
        return nb[:, pl.ds(pl.multiple_of(tt * S, S), S)]

    def share(m, cc):
        return jnp.bitwise_xor(y, m) * 2 + cc

    mine = normed_share(t)
    leaving = [j for unit in (0,) + SENDING for j in range(unit * b, unit * b + b) if j > 0]
    for j in leaving:
        k = chunk_of[j]
        placed = placing(j)
        out[j] = dot(placed, mine).astype(BF16)
        send(out.at[j], X.at[t, j], a2a_s.at[0, j], a2a_r.at[k], ep_peer(j))
        if k == 1:
            for m in range(1, NY):
                other = out1.at[m, j - b]
                other[...] = dot(placed, normed_share(share(m, c))).astype(BF16)
                send(other, X.at[share(m, c), j], a2a_s.at[m, j], a2a_r1.at[m], ep_peer(j))

    first = placing(0)
    for tt in range(T):
        X[tt, 0] = dot(first, nb[:, tt * S : (tt + 1) * S]).astype(BF16)

    def span(k):
        j0, n = blocks[k]
        return pl.ds(1, n - 1) if k == 0 else pl.ds(j0, n)

    def local_only(k):
        return blocks[k][0] == 0 and blocks[k][1] == 1

    def forward(k):
        if local_only(k):
            return
        block = X.at[t, span(k)]
        arrive(block, a2a_r.at[k])
        if k != 1:
            for m in range(1, NY):
                send(block, block, yg_s.at[m, k], yg_r.at[m, k], y_peer(m))
        send(block, block, cg_s.at[0, k], cg_r.at[0, k], core_peer)

    def forward_core(k):
        if local_only(k):
            return
        for m in range(1, NY):
            block = X.at[share(m, c), span(k)]
            arrive(block, a2a_r1.at[m] if k == 1 else yg_r.at[m, k])
            send(block, block, cg_s.at[m, k], cg_r.at[m, k], core_peer)

    def ready(k):
        if local_only(k):
            return
        for m in range(NY):
            arrive(X.at[share(m, 1 - c), span(k)], cg_r.at[m, k])

    NT = min(512, U)
    NS = min(256, S)

    def span_rows(k):
        j0, n = blocks[k]
        return pl.ds(j0 * C, n * C)

    def gate_up(k):
        j0, n = blocks[k]

        def body(i, carry):
            at = pl.ds(pl.multiple_of(i * NT, NT), NT)
            gate = up = None
            for tt in range(T):
                r = X[tt, j0 : j0 + n].reshape(n * C, S)
                deep = slice(tt * S, (tt + 1) * S)
                g = dot(r, wg_v[deep, at])
                u = dot(r, wu_v[deep, at])
                gate = g if gate is None else gate + g
                up = u if up is None else up + u
            hid[0 : n * C, at] = (silu(gate) * up).astype(BF16)
            return carry

        lax.fori_loop(0, U // NT, body, 0)

    def down(k):
        rs = span_rows(k)
        size = blocks[k][1] * C
        for mine_side in (False, True):
            core = c if mine_side else 1 - c
            for m in list(range(1, NY)) + [0]:
                base = share(m, core) * S
                for n in range(S // NS):
                    at = pl.ds(pl.multiple_of(base + n * NS, NS), NS)
                    part = dot(hid[0:size], wd_v[:, at])
                    if mine_side:
                        own[m, rs, n * NS : (n + 1) * NS] = part
                    else:
                        tc[m, rs, n * NS : (n + 1) * NS] = part.astype(BF16)
                if not mine_side:
                    send(tc.at[m, rs], fc.at[m, rs], rc_s.at[m, k], rc_r.at[m, k], core_peer)

    def reduce_core(k):
        rs = span_rows(k)
        for m in list(range(1, NY)) + [0]:
            arrive(fc.at[m, rs], rc_r.at[m, k])
            total = own[m, rs] + fc[m, rs].astype(F32)
            if m == 0:
                own[0, rs] = total
            else:
                ys[m, rs] = total.astype(BF16)
                send(ys.at[m, rs], yr.at[m, rs], ry_s.at[m, k], ry_r.at[m, k], y_peer(m))

    def reduce_y(k):
        j0, n = blocks[k]
        rs = span_rows(k)
        total = own[0, rs]
        for m in range(1, NY):
            arrive(yr.at[m, rs], ry_r.at[m, k])
            total = total + yr[m, rs].astype(F32)
        done = total.astype(BF16).reshape(n, C, S)
        for i in range(n):
            j = j0 + i
            if j == 0:
                ret[0] = done[0]
            else:
                fin[j] = done[i]
                send(fin.at[j], ret.at[j], rt_s.at[j], rt_r.at[k], ep_peer(j))

    def combine(k, place):
        if not local_only(k):
            arrive(ret.at[span(k)], rt_r.at[k])
        j0, n = blocks[k]
        size = n * C
        block = ret[j0 : j0 + n].reshape(size, S)
        lane = (lax.broadcasted_iota(jnp.int32, (tok, size), 1) + j0 * C).astype(F32)
        total = None
        for p in range(TOPK):
            chosen = (lane == cols_v[:, p : p + 1]).astype(BF16)
            term = dot(chosen, block) * cols_v[:, TOPK + p : TOPK + p + 1]
            total = term if total is None else total + term
        if place != "first":
            total = total + acc[...]
        if place != "last":
            acc[...] = total
        else:
            outb_ref[...] = total.astype(BF16)

    causal = row_i >= col_i

    def conv(ref, k_ref, start, size, rim_start):
        joined[0:HALO, 0:size] = rim[:, rim_start : rim_start + size].astype(F32)
        joined[HALO : HALO + rows, 0:size] = ref[:, start : start + size].astype(F32)
        kernel = k_ref[:, start : start + size].astype(F32)
        total = None
        for j in range(taps):
            at = HALO - taps + 1 + j
            term = kernel[j : j + 1] * joined[at : at + rows, 0:size]
            total = term if total is None else total + term
        return silu(total)

    def column(ref):
        index = lax.broadcasted_iota(jnp.int32, (heads, rows), 0)
        value = jnp.zeros((heads, rows), F32)
        for h in range(heads):
            value = jnp.where(index == h, ref[h], value)
        return value

    mix = {}
    lane128 = lax.broadcasted_iota(jnp.int32, (rows, LANES), 1)

    def mix_prepare():
        z = pre_v[...] + column(offset_s)
        step_t = jnp.maximum(z, 0.0) + jnp.log1p(jnp.exp(-jnp.abs(z)))
        decay_t = -jnp.exp(column(speed_s)) * step_t + extra_v[...]
        tri = causal.astype(F32)
        eye = (row_i == col_i).astype(F32)
        run = dot_last(tri, decay_t, HIGHEST)
        last = run[rows - 1 : rows]
        grown_v[...] = jnp.exp(run)
        dec_row = widen(jnp.exp(last), 0, heads, 1)
        dec_v[...] = jnp.broadcast_to(dec_row, dec_v.shape)
        mix["run"] = run
        mix["run_t"] = dot_last(decay_t, tri, HIGHEST)
        mix["step"] = dot_last(eye, step_t, HIGHEST)
        mix["to_end"] = jnp.exp(last - run)

        @pl.when(e > 0)
        def _():
            for i in range(3):
                arrive(rims[i][1], rim_r.at[i])

    def ssd(g):
        run, run_t, step, to_end = (mix[n] for n in ("run", "run_t", "step", "to_end"))
        lead = g * members
        cols = slice(g * wide, (g + 1) * wide)
        xc = conv(x_v, kx_v, g * wide, wide, g * wide)
        bb = conv(b_v, kb_v, g * STATE, STATE, channels + g * STATE).astype(BF16)
        cc = conv(c_v, kc_v, g * STATE, STATE, channels + latent + g * STATE).astype(BF16)
        cc_v[:, g * STATE : (g + 1) * STATE] = cc
        xs = xc * widen(step, lead, members, rows)
        xs16 = xs.astype(BF16)
        scores = dot_last(cc, bb)
        scores = jnp.where(causal, scores, 0.0)
        inside = []
        skip = []
        for pair in range(0, members, 2):
            x_pair = xs16[:, pair * HEAD_DIM : (pair + 2) * HEAD_DIM]
            both = []
            for h in (lead + pair, lead + pair + 1):
                gap = jnp.minimum(run[:, h : h + 1] - run_t[h : h + 1, :], 0.0)
                weights = (jnp.exp(gap) * scores).astype(BF16)
                both.append(dot(weights, x_pair))
            inside.append(jnp.where(lane128 < HEAD_DIM, both[0], both[1]))
            h = lead + pair
            skip.append(jnp.where(lane128 < HEAD_DIM, bypass_s[h], bypass_s[h + 1]))
        ybuf[:, cols] = jnp.concatenate(inside, axis=1) + xc * jnp.concatenate(skip, axis=1)
        x_end = (xs * widen(to_end, lead, members, rows)).astype(BF16)
        state[:, cols] = lax.dot_general(
            bb, x_end, (((0,), (0,)), ((), ())), preferred_element_type=F32
        )

    side = lax.rem(e, 2)
    group = lax.div(e, 2)
    pairs_count = E // 2

    def state_exchange():
        st16[0] = state[0:half].astype(BF16)
        st16[1] = state[half:STATE].astype(BF16)
        send(st16.at[1 - side], peerst, st_s.at[0], st_r.at[0], ep_peer(1))
        send(dec_v, peerdec, st_s.at[1], st_r.at[1], ep_peer(1))

    behind = (jnp.maximum(e - 2, 0), t)
    ahead = (jnp.minimum(e + 2, E - 1), t)

    def chain(low, high):
        @pl.when((group >= low) & (group < high))
        def _():
            arrive(peerst, st_r.at[0])
            arrive(peerdec, st_r.at[1])
            own_half = st16[side].astype(F32)
            other = peerst[...].astype(F32)
            own_dec = dec_v[0:1]
            other_dec = peerdec[0:1]
            left = side == 0
            s0 = jnp.where(left, own_half, other)
            s1 = jnp.where(left, other, own_half)
            d0 = jnp.where(left, own_dec, other_dec)
            d1 = jnp.where(left, other_dec, own_dec)

            @pl.when(group > 0)
            def _():
                arrive(chin, st_r.at[2])

            @pl.when(group == 0)
            def _():
                chin[...] = jnp.zeros(chin.shape, BF16)

            e0 = chin[...].astype(F32)
            e1 = e0 * d0 + s0

            @pl.when(group < pairs_count - 1)
            def _():
                chout[...] = (e1 * d1 + s1).astype(BF16)
                rcopy(chout, chin, st_s.at[2], st_r.at[2], ahead).start()

            enter[side] = jnp.where(left, e0, e1).astype(BF16)
            esend[...] = jnp.where(left, e1, e0).astype(BF16)
            rcopy(esend, enter.at[side], st_s.at[3], st_r.at[3], ep_peer(1)).start()

    def gate_norm():
        arrive(enter.at[1 - side], st_r.at[3])
        entered = enter[...].reshape(STATE, channels)
        for g in range(groups):
            cols = slice(g * wide, (g + 1) * wide)
            carried = dot(cc_v[:, g * STATE : (g + 1) * STATE], entered[:, cols])
            ssd_out = ybuf[:, cols] + carried * widen(grown_v[...], g * members, members, rows)
            gated = ssd_out * silu(valve_v[:, cols].astype(F32))
            norm = lax.rsqrt(jnp.mean(gated * gated, axis=1, keepdims=True) + NORM_EPS)
            normed[:, cols] = (gated * norm * again_v[cols].astype(F32)[None, :]).astype(BF16)

    width_a = wr_v.shape[1]
    NA = min(512, width_a)
    R = rows // T

    def project():
        for n in range(width_a // NA):
            part = dot(normed[...], wr_v[:, n * NA : (n + 1) * NA])
            for yy in range(NY):
                m = jnp.bitwise_xor(y, yy)
                low = part[(yy * 2) * R : (yy * 2 + 1) * R]
                high = part[(yy * 2 + 1) * R : (yy * 2 + 2) * R]
                aown[m, :, n * NA : (n + 1) * NA] = jnp.where(c == 0, low, high)
                atc[m, :, n * NA : (n + 1) * NA] = jnp.where(c == 0, high, low).astype(BF16)
        for m in list(range(1, NY)) + [0]:
            send(atc.at[m], afc.at[m], mc_s.at[m], mc_r.at[m], core_peer)

    def mix_core():
        for m in list(range(1, NY)) + [0]:
            arrive(afc.at[m], mc_r.at[m])
            total = aown[m] + afc[m].astype(F32)
            if m == 0:
                aown[0] = total
            else:
                ays[m] = total.astype(BF16)
                send(ays.at[m], ayr.at[m], my_s.at[m], my_r.at[m], y_peer(m))

    def mix_y():
        total = aown[0]
        for m in range(1, NY):
            arrive(ayr.at[m], my_r.at[m])
            total = total + ayr[m].astype(F32)
        outa_ref[...] = total.astype(BF16)

    bounds = [round(i * pairs_count / 4) for i in range(5)]
    seen = []

    def load_weights():
        for i in (12, 13, 14):
            loads[i].wait()

    def load_rest():
        for i in (15, 16, 17):
            loads[i].wait()

    def ssd_part(i):
        for g in range(i * groups // 4, (i + 1) * groups // 4):
            ssd(g)

    def chain_part(i):
        chain(bounds[i], bounds[i + 1])

    def combine_part(k):
        seen.append(k)
        place = "first" if len(seen) == 1 else "last" if len(seen) == len(blocks) else "add"
        combine(k, place)

    steps = {
        "fw": forward,
        "fc": forward_core,
        "rd": ready,
        "gu": gate_up,
        "dn": down,
        "rc": reduce_core,
        "ry": reduce_y,
        "cb": combine_part,
        "mp": mix_prepare,
        "ssd": ssd_part,
        "sx": state_exchange,
        "ch": chain_part,
        "lw": load_weights,
        "lr": load_rest,
        "gn": gate_norm,
        "pj": project,
        "mc": mix_core,
        "my": mix_y,
    }
    for name, *which in ORDER:
        with jax.named_scope(name + "".join(str(i) for i in which)):
            steps[name](*which)

    with jax.named_scope("drain"):
        for copy in sends:
            copy.wait_send()

    @pl.when(e < E - 1)
    def _():
        for i in range(3):
            rim_copy(i).wait_send()

    @pl.when(group < pairs_count - 1)
    def _():
        rcopy(chout, chin, st_s.at[2], st_r.at[2], ahead).wait_send()

    rcopy(esend, enter.at[side], st_s.at[3], st_r.at[3], ep_peer(1)).wait_send()


def local(
    blender_incoming_features,
    entry_latent_matrix,
    exit_latent_matrix,
    unactivated_valve,
    presoftplus_strides,
    extra_attenuation,
    incoming_feature_kernel,
    entry_latent_kernel,
    exit_latent_kernel,
    stride_offset_vector,
    attenuation_speed_exponent,
    bypass_coef_vector,
    cluster_rescale_coefs,
    blender_result_matrix,
    latter_microbatch_activations,
    specialist_rescale_coefs,
    specialist_valve_matrix,
    specialist_expand_matrix,
    specialist_contract_matrix,
    specialist_picks,
    selected_specialist_coefs,
):
    E = lax.axis_size("ep")
    T = lax.axis_size("tp")
    NY = T // 2
    rows, channels = blender_incoming_features.shape
    latent = entry_latent_matrix.shape[1]
    heads = presoftplus_strides.shape[1]
    taps = incoming_feature_kernel.shape[0]
    wide = channels // (latent // STATE)
    half = STATE // 2
    tok, width = latter_microbatch_activations.shape
    S = width // T
    C = 3 * tok * TOPK // (2 * E)
    b = E // UNITS
    wg, wu, wd = specialist_valve_matrix[0], specialist_expand_matrix[0], specialist_contract_matrix[0]
    U = wg.shape[1]
    width_a = blender_result_matrix.shape[1]
    R = rows // T
    far = [
        specialist_picks.T,
        selected_specialist_coefs.T,
        latter_microbatch_activations,
        specialist_rescale_coefs,
        blender_incoming_features,
        entry_latent_matrix,
        exit_latent_matrix,
        incoming_feature_kernel,
        entry_latent_kernel,
        exit_latent_kernel,
        presoftplus_strides.T,
        extra_attenuation.T,
        unactivated_valve,
        cluster_rescale_coefs,
        wg,
        wu,
        wd,
        blender_result_matrix,
    ]
    near = [stride_offset_vector, attenuation_speed_exponent, bypass_coef_vector]
    landing = [pltpu.VMEM(a.shape, a.dtype) for a in far]
    dma = pltpu.SemaphoreType.DMA
    vmem = pltpu.VMEM
    return pl.pallas_call(
        functools.partial(layer_kernel, E, T),
        in_specs=[pl.BlockSpec(memory_space=pl.ANY)] * len(far)
        + [pl.BlockSpec(memory_space=pltpu.SMEM)] * len(near),
        out_specs=[pl.BlockSpec(memory_space=pltpu.VMEM)] * 2,
        out_shape=[pltpu.VMEM((R, width_a), BF16), pltpu.VMEM((tok, S), BF16)],
        scratch_shapes=landing
        + [
            vmem((tok, width), BF16),
            vmem((E, C, S), BF16),
            vmem((NY, b, C, S), BF16),
            vmem((T, E, C, S), BF16),
            vmem((max(n for _, n in GROUPS) * b * C, U), BF16),
            vmem((NY, E * C, S), BF16),
            vmem((NY, E * C, S), BF16),
            vmem((NY, E * C, S), F32),
            vmem((NY, E * C, S), BF16),
            vmem((NY, E * C, S), BF16),
            vmem((E, C, S), BF16),
            vmem((E, C, S), BF16),
            vmem((tok, S), F32),
            vmem((tok, 8), F32),
            vmem((HALO, channels + 2 * latent), BF16),
            vmem((rows + HALO, wide), F32),
            vmem((rows, channels), F32),
            vmem((rows, latent), BF16),
            vmem((rows, heads), F32),
            vmem((STATE, channels), F32),
            vmem((2, half, channels), BF16),
            vmem((half, channels), BF16),
            vmem((8, channels), F32),
            vmem((8, channels), F32),
            vmem((half, channels), BF16),
            vmem((half, channels), BF16),
            vmem((2, half, channels), BF16),
            vmem((half, channels), BF16),
            vmem((rows, channels), BF16),
            vmem((NY, R, width_a), BF16),
            vmem((NY, R, width_a), BF16),
            vmem((NY, R, width_a), F32),
            vmem((NY, R, width_a), BF16),
            vmem((NY, R, width_a), BF16),
            dma((len(far),)),
            dma((NY, E)),
            dma((UNITS,)),
            dma((NY,)),
            dma((NY, UNITS)),
            dma((NY, UNITS)),
            dma((NY, UNITS)),
            dma((NY, UNITS)),
            dma((NY, UNITS)),
            dma((NY, UNITS)),
            dma((NY, UNITS)),
            dma((NY, UNITS)),
            dma((E,)),
            dma((UNITS,)),
            dma((NY,)),
            dma((NY,)),
            dma((NY,)),
            dma((NY,)),
            dma((3,)),
            dma((3,)),
            dma((4,)),
            dma((4,)),
        ],
        compiler_params=pltpu.CompilerParams(
            collective_id=0, has_side_effects=True, vmem_limit_bytes=60 * 1024 * 1024
        ),
        name="layer",
    )(*far, *near)


def solution(mesh):
    in_specs = (
        P("ep", "tp"),
        P("ep", "tp"),
        P("ep", "tp"),
        P("ep", "tp"),
        P("ep", "tp"),
        P("ep", "tp"),
        P(None, "tp"),
        P(None, "tp"),
        P(None, "tp"),
        P("tp"),
        P("tp"),
        P("tp"),
        P("tp"),
        P("tp", None),
        P("ep", None),
        P(),
        P("ep", None, "tp"),
        P("ep", None, "tp"),
        P("ep", "tp", None),
        P("ep", None),
        P("ep", None),
    )
    out_specs = (P(("ep", "tp"), None), P("ep", "tp"))
    return jax.shard_map(local, mesh=mesh, in_specs=in_specs, out_specs=out_specs, check_vma=False)
```

```python
import functools

import jax
import jax.numpy as jnp
from jax import lax
from jax.experimental import pallas as pl
from jax.experimental.pallas import tpu as pltpu
from jax.sharding import PartitionSpec as P

HEADS = 64
HEAD_DIM = 64
SHARING_CLUSTERS = 16
STATE = 128
TOPK = 2

NORM_EPS = 1e-06
HIGHEST = lax.Precision.HIGHEST
MESH = pl.DeviceIdType.MESH
F32 = jnp.float32
BF16 = jnp.bfloat16
HALO = 16
LANES = 128
UNITS = 8
GROUPS = ((0, 1), (1, 1), (2, 2), (4, 1), (5, 1), (6, 1), (7, 1))
KINDS = ("out", "out1", "y", "core", "tc", "ys", "fin", "rim", "st16", "dec", "chain", "enter", "atc", "ays")
TWICE = 1
SENDING = (2, 4, 1, 5, 3, 7, 6)

ORDER = (
    ("rd", 0),
    ("lw",),
    ("gu", 0),
    ("mp",),
    ("fw", 2),
    ("ssd", 0),
    ("fw", 4),
    ("ssd", 1),
    ("fc", 1),
    ("fw", 1),
    ("ssd", 2),
    ("ssd", 3),
    ("sx",),
    ("fc", 4),
    ("rd", 1),
    ("fw", 3),
    ("dn", 0),
    ("fw", 5),
    ("gu", 1),
    ("rd", 4),
    ("ch", 0),
    ("rc", 0),
    ("dn", 1),
    ("gu", 4),
    ("rc", 1),
    ("fc", 5),
    ("dn", 4),
    ("fc", 2),
    ("fw", 6),
    ("ch", 1),
    ("rd", 5),
    ("fc", 3),
    ("gu", 5),
    ("rc", 4),
    ("dn", 5),
    ("fw", 7),
    ("rd", 2),
    ("gu", 2),
    ("fc", 6),
    ("rc", 5),
    ("ch", 2),
    ("ry", 1),
    ("dn", 2),
    ("rd", 6),
    ("ry", 4),
    ("gu", 6),
    ("dn", 6),
    ("fc", 7),
    ("ch", 3),
    ("rc", 6),
    ("ry", 0),
    ("ry", 5),
    ("rc", 2),
    ("rd", 7),
    ("gu", 7),
    ("dn", 7),
    ("lr",),
    ("gn",),
    ("rc", 7),
    ("ry", 6),
    ("cb", 1),
    ("pj",),
    ("ry", 2),
    ("cb", 5),
    ("mc",),
    ("ry", 7),
    ("cb", 6),
    ("cb", 0),
    ("cb", 4),
    ("cb", 2),
    ("my",),
    ("cb", 7),
)


def silu(v):
    return v / (1.0 + jnp.exp(-v))


def dot(a, b):
    return jnp.dot(a, b, preferred_element_type=F32)


def dot_last(a, b, precision=None):
    return lax.dot_general(
        a, b, (((1,), (1,)), ((), ())), preferred_element_type=F32, precision=precision
    )


def widen(per_head, first, count, rows):
    lane = lax.broadcasted_iota(jnp.int32, (rows, LANES), 1)
    pieces = []
    for h in range(first, first + count, 2):
        left = jnp.broadcast_to(per_head[:, h : h + 1], (rows, LANES))
        right = jnp.broadcast_to(per_head[:, h + 1 : h + 2], (rows, LANES))
        pieces.append(jnp.where(lane < HEAD_DIM, left, right))
    return jnp.concatenate(pieces, axis=1)


def layer_kernel(
    E,
    T,
    picks_h,
    coefs_h,
    act_h,
    bgain_h,
    x_h,
    b_h,
    c_h,
    kx_h,
    kb_h,
    kc_h,
    pre_h,
    extra_h,
    valve_h,
    again_h,
    wg_h,
    wu_h,
    wd_h,
    wr_h,
    offset_s,
    speed_s,
    bypass_s,
    outa_ref,
    outb_ref,
    picks_v,
    coefs_v,
    act_v,
    bgain_v,
    x_v,
    b_v,
    c_v,
    kx_v,
    kb_v,
    kc_v,
    pre_v,
    extra_v,
    valve_v,
    again_v,
    wg_v,
    wu_v,
    wd_v,
    wr_v,
    nb,
    out,
    out1,
    X,
    hid,
    tc,
    fc,
    own,
    ys,
    yr,
    fin,
    ret,
    acc,
    cols_v,
    rim,
    joined,
    ybuf,
    cc_v,
    grown_v,
    state,
    st16,
    peerst,
    dec_v,
    peerdec,
    chin,
    chout,
    enter,
    esend,
    normed,
    atc,
    afc,
    aown,
    ays,
    ayr,
    load_sem,
    sent,
    out_r,
    y_r,
    core_r,
    sum_r,
    ysum_r,
    ret_r,
    once_r,
    state_r,
):
    e = lax.axis_index("ep")
    t = lax.axis_index("tp")
    y = lax.div(t, 2)
    c = lax.rem(t, 2)
    NY = T // 2
    b = E // UNITS
    blocks = {first: (first * b, count * b) for first, count in GROUPS}
    units = {first: range(first, first + count) for first, count in GROUPS}
    tok, width = act_v.shape
    S = width // T
    C = out.shape[1]
    rows, channels = x_v.shape
    latent = b_v.shape[1]
    heads = pre_v.shape[0]
    groups = latent // STATE
    members = heads // groups
    wide = members * HEAD_DIM
    taps = kx_v.shape[0]
    half = STATE // 2
    U = wg_v.shape[1]

    pairs = [
        (picks_h, picks_v),
        (coefs_h, coefs_v),
        (act_h, act_v),
        (bgain_h, bgain_v),
        (x_h, x_v),
        (b_h, b_v),
        (c_h, c_v),
        (kx_h, kx_v),
        (kb_h, kb_v),
        (kc_h, kc_v),
        (pre_h, pre_v),
        (extra_h, extra_v),
        (wg_h, wg_v),
        (wu_h, wu_v),
        (wd_h, wd_v),
        (valve_h, valve_v),
        (again_h, again_v),
        (wr_h, wr_v),
    ]
    loads = {}
    for i, (src, dst) in enumerate(pairs):
        loads[i] = pltpu.make_async_copy(src, dst, load_sem.at[i])
        loads[i].start()

    def ep_peer(j):
        return (jnp.bitwise_xor(e, j), t)

    def y_peer(m):
        return (e, jnp.bitwise_xor(y, m) * 2 + c)

    core_peer = (e, y * 2 + 1 - c)

    barrier = pltpu.get_barrier_semaphore()
    peers = [ep_peer(j) for j in range(1, E)] + [y_peer(m) for m in range(1, NY)] + [core_peer]
    for peer in peers:
        pl.semaphore_signal(barrier, inc=1, device_id=peer, device_id_type=MESH)

    def rcopy(src, dst, ssem, rsem, dev):
        return pltpu.make_async_remote_copy(
            src_ref=src,
            dst_ref=dst,
            send_sem=ssem,
            recv_sem=rsem,
            device_id=dev,
            device_id_type=MESH,
        )

    def send(src, dst, kind, rsem, dev):
        rcopy(src, dst, sent.at[KINDS.index(kind)], rsem, dev).start()

    def drain(kind, whole):
        rcopy(whole, whole, sent.at[KINDS.index(kind)], state_r.at[0], core_peer).wait_send()

    def arrive(dst, rsem):
        rcopy(dst, dst, sent.at[0], rsem, core_peer).wait_recv()

    index_of = {k: i for i, k in enumerate(blocks)}
    others = pl.ds(1, NY - 1)
    every = pl.ds(0, NY)

    with jax.named_scope("load_b"):
        for i in range(4):
            loads[i].wait()
    pick = jnp.bitwise_xor(picks_v[...], e)
    expert = lax.broadcasted_iota(jnp.int32, (E, tok), 0)
    row_i = lax.broadcasted_iota(jnp.int32, (tok, tok), 0)
    col_i = lax.broadcasted_iota(jnp.int32, (tok, tok), 1)
    before = (row_i < col_i).astype(BF16)
    hot0 = (expert == pick[0:1]).astype(F32)
    hot1 = (expert == pick[1:2]).astype(F32)
    cum0 = dot(hot0.astype(BF16), before)
    cum1 = dot(hot1.astype(BF16), before) + jnp.sum(hot0, axis=1, keepdims=True)
    rank0 = jnp.sum(hot0 * cum0, axis=0, keepdims=True)
    rank1 = jnp.sum(hot1 * cum1, axis=0, keepdims=True)
    slot0 = pick[0:1].astype(F32) * float(C) + rank0
    slot1 = pick[1:2].astype(F32) * float(C) + rank1
    stacked = jnp.concatenate(
        [slot0, slot1, coefs_v[...], jnp.zeros((4, tok), F32)], axis=0
    )
    cols_v[...] = stacked.T

    wide_act = act_v[...].astype(F32)
    scale = lax.rsqrt(jnp.mean(wide_act * wide_act, axis=1, keepdims=True) + NORM_EPS)
    nb[...] = (wide_act * scale * bgain_v[...].astype(F32)[None, :]).astype(BF16)

    def placing(j):
        slot = (lax.broadcasted_iota(jnp.int32, (C, tok), 0) + j * C).astype(F32)
        return ((slot == slot0) | (slot == slot1)).astype(BF16)

    with jax.named_scope("load_a"):
        for i in range(4, 12):
            loads[i].wait()
    with jax.named_scope("barrier"):
        pl.semaphore_wait(barrier, len(peers))
    tail = pl.ds(rows - HALO, HALO)
    rims = [
        (x_v.at[tail], rim.at[:, pl.ds(0, channels)]),
        (b_v.at[tail], rim.at[:, pl.ds(channels, latent)]),
        (c_v.at[tail], rim.at[:, pl.ds(channels + latent, latent)]),
    ]
    following = (jnp.minimum(e + 1, E - 1), t)

    @pl.when(e < E - 1)
    def _():
        for src, dst in rims:
            send(src, dst, "rim", once_r.at[1], following)

    @pl.when(e == 0)
    def _():
        rim[...] = jnp.zeros(rim.shape, BF16)

    def normed_share(tt):
        return nb[:, pl.ds(pl.multiple_of(tt * S, S), S)]

    def share(m, cc):
        return jnp.bitwise_xor(y, m) * 2 + cc

    mine = normed_share(t)
    leaving = [j for unit in (0,) + SENDING for j in range(unit * b, unit * b + b) if j > 0]
    for j in leaving:
        u = j // b
        placed = placing(j)
        out[j] = dot(placed, mine).astype(BF16)
        send(out.at[j], X.at[t, j], "out", out_r.at[u], ep_peer(j))
        if u == TWICE:
            for m in range(1, NY):
                other = out1.at[m, j - TWICE * b]
                other[...] = dot(placed, normed_share(share(m, c))).astype(BF16)
                send(other, X.at[share(m, c), j], "out1", once_r.at[0], ep_peer(j))

    first = placing(0)
    for tt in range(T):
        X[tt, 0] = dot(first, nb[:, tt * S : (tt + 1) * S]).astype(BF16)

    def span(k):
        j0, n = blocks[k]
        return pl.ds(1, n - 1) if k == 0 else pl.ds(j0, n)

    def unit(u):
        return pl.ds(1, b - 1) if u == 0 else pl.ds(u * b, b)

    def local_only(k):
        return blocks[k][0] == 0 and blocks[k][1] == 1

    def forward(u):
        block = X.at[t, unit(u)]
        arrive(block, out_r.at[u])
        if u != TWICE:
            for m in range(1, NY):
                send(block, block, "y", y_r.at[u], y_peer(m))
        send(block, block, "core", core_r.at[u], core_peer)

    def forward_core(u):
        arrive(X.at[pl.ds(0, NY - 1), unit(u)], once_r.at[0] if u == TWICE else y_r.at[u])
        for m in range(1, NY):
            block = X.at[share(m, c), unit(u)]
            send(block, block, "core", core_r.at[u], core_peer)

    def ready(k):
        if k == 0 and b > 1:
            forward(0)
            forward_core(0)
        for u in units[k]:
            if u > 0 or b > 1:
                arrive(X.at[every, unit(u)], core_r.at[u])

    NT = min(512, U)
    NS = min(256, S)

    def span_rows(k):
        j0, n = blocks[k]
        return pl.ds(j0 * C, n * C)

    def gate_up(k):
        j0, n = blocks[k]

        def body(i, carry):
            at = pl.ds(pl.multiple_of(i * NT, NT), NT)
            gate = up = None
            for tt in range(T):
                r = X[tt, j0 : j0 + n].reshape(n * C, S)
                deep = slice(tt * S, (tt + 1) * S)
                g = dot(r, wg_v[deep, at])
                u = dot(r, wu_v[deep, at])
                gate = g if gate is None else gate + g
                up = u if up is None else up + u
            hid[0 : n * C, at] = (silu(gate) * up).astype(BF16)
            return carry

        lax.fori_loop(0, U // NT, body, 0)

    def down(k):
        rs = span_rows(k)
        size = blocks[k][1] * C
        for mine_side in (False, True):
            core = c if mine_side else 1 - c
            for m in list(range(1, NY)) + [0]:
                base = share(m, core) * S
                for n in range(S // NS):
                    at = pl.ds(pl.multiple_of(base + n * NS, NS), NS)
                    part = dot(hid[0:size], wd_v[:, at])
                    if mine_side:
                        own[m, rs, n * NS : (n + 1) * NS] = part
                    else:
                        tc[m, rs, n * NS : (n + 1) * NS] = part.astype(BF16)
                if not mine_side:
                    send(tc.at[m, rs], fc.at[m, rs], "tc", sum_r.at[index_of[k]], core_peer)

    def reduce_core(k):
        rs = span_rows(k)
        arrive(fc.at[every, rs], sum_r.at[index_of[k]])
        for m in list(range(1, NY)) + [0]:
            total = own[m, rs] + fc[m, rs].astype(F32)
            if m == 0:
                own[0, rs] = total
            else:
                ys[m, rs] = total.astype(BF16)
                send(ys.at[m, rs], yr.at[m, rs], "ys", ysum_r.at[index_of[k]], y_peer(m))

    def reduce_y(k):
        j0, n = blocks[k]
        rs = span_rows(k)
        total = own[0, rs]
        arrive(yr.at[others, rs], ysum_r.at[index_of[k]])
        for m in range(1, NY):
            total = total + yr[m, rs].astype(F32)
        done = total.astype(BF16).reshape(n, C, S)
        for i in range(n):
            j = j0 + i
            if j == 0:
                ret[0] = done[0]
            else:
                fin[j] = done[i]
                send(fin.at[j], ret.at[j], "fin", ret_r.at[index_of[k]], ep_peer(j))

    def combine(k, place):
        if not local_only(k):
            arrive(ret.at[span(k)], ret_r.at[index_of[k]])
        j0, n = blocks[k]
        size = n * C
        block = ret[j0 : j0 + n].reshape(size, S)
        lane = (lax.broadcasted_iota(jnp.int32, (tok, size), 1) + j0 * C).astype(F32)
        total = None
        for p in range(TOPK):
            chosen = (lane == cols_v[:, p : p + 1]).astype(BF16)
            term = dot(chosen, block) * cols_v[:, TOPK + p : TOPK + p + 1]
            total = term if total is None else total + term
        if place != "first":
            total = total + acc[...]
        if place != "last":
            acc[...] = total
        else:
            outb_ref[...] = total.astype(BF16)

    causal = row_i >= col_i

    def conv(ref, k_ref, start, size, rim_start):
        joined[0:HALO, 0:size] = rim[:, rim_start : rim_start + size].astype(F32)
        joined[HALO : HALO + rows, 0:size] = ref[:, start : start + size].astype(F32)
        kernel = k_ref[:, start : start + size].astype(F32)
        total = None
        for j in range(taps):
            at = HALO - taps + 1 + j
            term = kernel[j : j + 1] * joined[at : at + rows, 0:size]
            total = term if total is None else total + term
        return silu(total)

    def column(ref):
        index = lax.broadcasted_iota(jnp.int32, (heads, rows), 0)
        value = jnp.zeros((heads, rows), F32)
        for h in range(heads):
            value = jnp.where(index == h, ref[h], value)
        return value

    mix = {}
    lane128 = lax.broadcasted_iota(jnp.int32, (rows, LANES), 1)

    def mix_prepare():
        z = pre_v[...] + column(offset_s)
        step_t = jnp.maximum(z, 0.0) + jnp.log1p(jnp.exp(-jnp.abs(z)))
        decay_t = -jnp.exp(column(speed_s)) * step_t + extra_v[...]
        tri = causal.astype(F32)
        eye = (row_i == col_i).astype(F32)
        run = dot_last(tri, decay_t, HIGHEST)
        last = run[rows - 1 : rows]
        grown_v[...] = jnp.exp(run)
        dec_row = widen(jnp.exp(last), 0, heads, 1)
        dec_v[...] = jnp.broadcast_to(dec_row, dec_v.shape)
        mix["run"] = run
        mix["run_t"] = dot_last(decay_t, tri, HIGHEST)
        mix["step"] = dot_last(eye, step_t, HIGHEST)
        mix["to_end"] = jnp.exp(last - run)

        @pl.when(e > 0)
        def _():
            arrive(rim, once_r.at[1])

    def ssd(g):
        run, run_t, step, to_end = (mix[n] for n in ("run", "run_t", "step", "to_end"))
        lead = g * members
        cols = slice(g * wide, (g + 1) * wide)
        xc = conv(x_v, kx_v, g * wide, wide, g * wide)
        bb = conv(b_v, kb_v, g * STATE, STATE, channels + g * STATE).astype(BF16)
        cc = conv(c_v, kc_v, g * STATE, STATE, channels + latent + g * STATE).astype(BF16)
        cc_v[:, g * STATE : (g + 1) * STATE] = cc
        xs = xc * widen(step, lead, members, rows)
        xs16 = xs.astype(BF16)
        scores = dot_last(cc, bb)
        scores = jnp.where(causal, scores, 0.0)
        inside = []
        skip = []
        for pair in range(0, members, 2):
            x_pair = xs16[:, pair * HEAD_DIM : (pair + 2) * HEAD_DIM]
            both = []
            for h in (lead + pair, lead + pair + 1):
                gap = jnp.minimum(run[:, h : h + 1] - run_t[h : h + 1, :], 0.0)
                weights = (jnp.exp(gap) * scores).astype(BF16)
                both.append(dot(weights, x_pair))
            inside.append(jnp.where(lane128 < HEAD_DIM, both[0], both[1]))
            h = lead + pair
            skip.append(jnp.where(lane128 < HEAD_DIM, bypass_s[h], bypass_s[h + 1]))
        ybuf[:, cols] = jnp.concatenate(inside, axis=1) + xc * jnp.concatenate(skip, axis=1)
        x_end = (xs * widen(to_end, lead, members, rows)).astype(BF16)
        state[:, cols] = lax.dot_general(
            bb, x_end, (((0,), (0,)), ((), ())), preferred_element_type=F32
        )

    side = lax.rem(e, 2)
    group = lax.div(e, 2)
    pairs_count = E // 2

    def state_exchange():
        st16[0] = state[0:half].astype(BF16)
        st16[1] = state[half:STATE].astype(BF16)
        send(st16.at[1 - side], peerst, "st16", state_r.at[0], ep_peer(1))
        send(dec_v, peerdec, "dec", state_r.at[1], ep_peer(1))

    behind = (jnp.maximum(e - 2, 0), t)
    ahead = (jnp.minimum(e + 2, E - 1), t)

    def chain(low, high):
        @pl.when((group >= low) & (group < high))
        def _():
            arrive(peerst, state_r.at[0])
            arrive(peerdec, state_r.at[1])
            own_half = st16[side].astype(F32)
            other = peerst[...].astype(F32)
            own_dec = dec_v[0:1]
            other_dec = peerdec[0:1]
            left = side == 0
            s0 = jnp.where(left, own_half, other)
            s1 = jnp.where(left, other, own_half)
            d0 = jnp.where(left, own_dec, other_dec)
            d1 = jnp.where(left, other_dec, own_dec)

            @pl.when(group > 0)
            def _():
                arrive(chin, state_r.at[2])

            @pl.when(group == 0)
            def _():
                chin[...] = jnp.zeros(chin.shape, BF16)

            e0 = chin[...].astype(F32)
            e1 = e0 * d0 + s0

            @pl.when(group < pairs_count - 1)
            def _():
                chout[...] = (e1 * d1 + s1).astype(BF16)
                send(chout, chin, "chain", state_r.at[2], ahead)

            enter[side] = jnp.where(left, e0, e1).astype(BF16)
            esend[...] = jnp.where(left, e1, e0).astype(BF16)
            send(esend, enter.at[side], "enter", state_r.at[3], ep_peer(1))

    def gate_norm():
        arrive(enter.at[1 - side], state_r.at[3])
        entered = enter[...].reshape(STATE, channels)
        for g in range(groups):
            cols = slice(g * wide, (g + 1) * wide)
            carried = dot(cc_v[:, g * STATE : (g + 1) * STATE], entered[:, cols])
            ssd_out = ybuf[:, cols] + carried * widen(grown_v[...], g * members, members, rows)
            gated = ssd_out * silu(valve_v[:, cols].astype(F32))
            norm = lax.rsqrt(jnp.mean(gated * gated, axis=1, keepdims=True) + NORM_EPS)
            normed[:, cols] = (gated * norm * again_v[cols].astype(F32)[None, :]).astype(BF16)

    width_a = wr_v.shape[1]
    NA = min(512, width_a)
    R = rows // T

    def project():
        for n in range(width_a // NA):
            part = dot(normed[...], wr_v[:, n * NA : (n + 1) * NA])
            for yy in range(NY):
                m = jnp.bitwise_xor(y, yy)
                low = part[(yy * 2) * R : (yy * 2 + 1) * R]
                high = part[(yy * 2 + 1) * R : (yy * 2 + 2) * R]
                aown[m, :, n * NA : (n + 1) * NA] = jnp.where(c == 0, low, high)
                atc[m, :, n * NA : (n + 1) * NA] = jnp.where(c == 0, high, low).astype(BF16)
        for m in list(range(1, NY)) + [0]:
            send(atc.at[m], afc.at[m], "atc", once_r.at[2], core_peer)

    def mix_core():
        arrive(afc, once_r.at[2])
        for m in list(range(1, NY)) + [0]:
            total = aown[m] + afc[m].astype(F32)
            if m == 0:
                aown[0] = total
            else:
                ays[m] = total.astype(BF16)
                send(ays.at[m], ayr.at[m], "ays", once_r.at[3], y_peer(m))

    def mix_y():
        total = aown[0]
        arrive(ayr.at[others], once_r.at[3])
        for m in range(1, NY):
            total = total + ayr[m].astype(F32)
        outa_ref[...] = total.astype(BF16)

    bounds = [round(i * pairs_count / 4) for i in range(5)]
    seen = []

    def load_weights():
        for i in (12, 13, 14):
            loads[i].wait()

    def load_rest():
        for i in (15, 16, 17):
            loads[i].wait()

    def ssd_part(i):
        for g in range(i * groups // 4, (i + 1) * groups // 4):
            ssd(g)

    def chain_part(i):
        chain(bounds[i], bounds[i + 1])

    def combine_part(k):
        seen.append(k)
        place = "first" if len(seen) == 1 else "last" if len(seen) == len(blocks) else "add"
        combine(k, place)

    steps = {
        "fw": forward,
        "fc": forward_core,
        "rd": ready,
        "gu": gate_up,
        "dn": down,
        "rc": reduce_core,
        "ry": reduce_y,
        "cb": combine_part,
        "mp": mix_prepare,
        "ssd": ssd_part,
        "sx": state_exchange,
        "ch": chain_part,
        "lw": load_weights,
        "lr": load_rest,
        "gn": gate_norm,
        "pj": project,
        "mc": mix_core,
        "my": mix_y,
    }
    for name, *which in ORDER:
        with jax.named_scope(name + "".join(str(i) for i in which)):
            steps[name](*which)

    with jax.named_scope("drain"):
        far = E - 1
        drain("out", out.at[pl.ds(1, far)])
        if TWICE > 0:
            drain("out1", out1.at[others])
            far -= b
        drain("y", X.at[pl.ds(0, NY - 1), pl.ds(0, far)])
        drain("core", X.at[every, pl.ds(1, E - 1)])
        drain("tc", tc)
        drain("ys", ys.at[others])
        drain("fin", fin.at[pl.ds(1, E - 1)])
        drain("st16", peerst)
        drain("dec", dec_v)
        drain("enter", esend)
        drain("atc", atc)
        drain("ays", ays.at[others])

        @pl.when(e < E - 1)
        def _():
            drain("rim", rim)

        @pl.when(group < pairs_count - 1)
        def _():
            drain("chain", chout)


def local(
    blender_incoming_features,
    entry_latent_matrix,
    exit_latent_matrix,
    unactivated_valve,
    presoftplus_strides,
    extra_attenuation,
    incoming_feature_kernel,
    entry_latent_kernel,
    exit_latent_kernel,
    stride_offset_vector,
    attenuation_speed_exponent,
    bypass_coef_vector,
    cluster_rescale_coefs,
    blender_result_matrix,
    latter_microbatch_activations,
    specialist_rescale_coefs,
    specialist_valve_matrix,
    specialist_expand_matrix,
    specialist_contract_matrix,
    specialist_picks,
    selected_specialist_coefs,
):
    E = lax.axis_size("ep")
    T = lax.axis_size("tp")
    NY = T // 2
    rows, channels = blender_incoming_features.shape
    latent = entry_latent_matrix.shape[1]
    heads = presoftplus_strides.shape[1]
    taps = incoming_feature_kernel.shape[0]
    wide = channels // (latent // STATE)
    half = STATE // 2
    tok, width = latter_microbatch_activations.shape
    S = width // T
    C = 3 * tok * TOPK // (2 * E)
    b = E // UNITS
    wg, wu, wd = specialist_valve_matrix[0], specialist_expand_matrix[0], specialist_contract_matrix[0]
    U = wg.shape[1]
    width_a = blender_result_matrix.shape[1]
    R = rows // T
    far = [
        specialist_picks.T,
        selected_specialist_coefs.T,
        latter_microbatch_activations,
        specialist_rescale_coefs,
        blender_incoming_features,
        entry_latent_matrix,
        exit_latent_matrix,
        incoming_feature_kernel,
        entry_latent_kernel,
        exit_latent_kernel,
        presoftplus_strides.T,
        extra_attenuation.T,
        unactivated_valve,
        cluster_rescale_coefs,
        wg,
        wu,
        wd,
        blender_result_matrix,
    ]
    near = [stride_offset_vector, attenuation_speed_exponent, bypass_coef_vector]
    landing = [pltpu.VMEM(a.shape, a.dtype) for a in far]
    dma = pltpu.SemaphoreType.DMA
    vmem = pltpu.VMEM
    return pl.pallas_call(
        functools.partial(layer_kernel, E, T),
        in_specs=[pl.BlockSpec(memory_space=pl.ANY)] * len(far)
        + [pl.BlockSpec(memory_space=pltpu.SMEM)] * len(near),
        out_specs=[pl.BlockSpec(memory_space=pltpu.VMEM)] * 2,
        out_shape=[pltpu.VMEM((R, width_a), BF16), pltpu.VMEM((tok, S), BF16)],
        scratch_shapes=landing
        + [
            vmem((tok, width), BF16),
            vmem((E, C, S), BF16),
            vmem((NY, b, C, S), BF16),
            vmem((T, E, C, S), BF16),
            vmem((max(n for _, n in GROUPS) * b * C, U), BF16),
            vmem((NY, E * C, S), BF16),
            vmem((NY, E * C, S), BF16),
            vmem((NY, E * C, S), F32),
            vmem((NY, E * C, S), BF16),
            vmem((NY, E * C, S), BF16),
            vmem((E, C, S), BF16),
            vmem((E, C, S), BF16),
            vmem((tok, S), F32),
            vmem((tok, 8), F32),
            vmem((HALO, channels + 2 * latent), BF16),
            vmem((rows + HALO, wide), F32),
            vmem((rows, channels), F32),
            vmem((rows, latent), BF16),
            vmem((rows, heads), F32),
            vmem((STATE, channels), F32),
            vmem((2, half, channels), BF16),
            vmem((half, channels), BF16),
            vmem((8, channels), F32),
            vmem((8, channels), F32),
            vmem((half, channels), BF16),
            vmem((half, channels), BF16),
            vmem((2, half, channels), BF16),
            vmem((half, channels), BF16),
            vmem((rows, channels), BF16),
            vmem((NY, R, width_a), BF16),
            vmem((NY, R, width_a), BF16),
            vmem((NY, R, width_a), F32),
            vmem((NY, R, width_a), BF16),
            vmem((NY, R, width_a), BF16),
            dma((len(far),)),
            dma((len(KINDS),)),
            dma((UNITS,)),
            dma((UNITS,)),
            dma((UNITS,)),
            dma((len(GROUPS),)),
            dma((len(GROUPS),)),
            dma((len(GROUPS),)),
            dma((4,)),
            dma((4,)),
        ],
        compiler_params=pltpu.CompilerParams(
            collective_id=0, has_side_effects=True, vmem_limit_bytes=60 * 1024 * 1024
        ),
        name="layer",
    )(*far, *near)


def solution(mesh):
    in_specs = (
        P("ep", "tp"),
        P("ep", "tp"),
        P("ep", "tp"),
        P("ep", "tp"),
        P("ep", "tp"),
        P("ep", "tp"),
        P(None, "tp"),
        P(None, "tp"),
        P(None, "tp"),
        P("tp"),
        P("tp"),
        P("tp"),
        P("tp"),
        P("tp", None),
        P("ep", None),
        P(),
        P("ep", None, "tp"),
        P("ep", None, "tp"),
        P("ep", "tp", None),
        P("ep", None),
        P("ep", None),
    )
    out_specs = (P(("ep", "tp"), None), P("ep", "tp"))
    return jax.shard_map(local, mesh=mesh, in_specs=in_specs, out_specs=out_specs, check_vma=False)
```

```python
import functools

import jax
import jax.numpy as jnp
from jax import lax
from jax.experimental import pallas as pl
from jax.experimental.pallas import tpu as pltpu
from jax.sharding import PartitionSpec as P

HEADS = 64
HEAD_DIM = 64
SHARING_CLUSTERS = 16
STATE = 128
TOPK = 2

NORM_EPS = 1e-06
HIGHEST = lax.Precision.HIGHEST
MESH = pl.DeviceIdType.MESH
F32 = jnp.float32
BF16 = jnp.bfloat16
HALO = 16
LANES = 128
UNITS = 8
GROUPS = ((0, 1), (1, 1), (2, 2), (4, 1), (5, 1), (6, 1), (7, 1))
KINDS = ("out", "out1", "y", "core", "tc", "ys", "fin", "rim", "st16", "dec", "chain", "enter", "atc", "ays")
TWICE = 1
SENDING = (2, 4, 1, 5, 6, 3, 7)

ORDER = (
    ("mp",),
    ("rd", 0),
    ("lw",),
    ("gu", 0),
    ("ld",),
    ("dn", 0),
    ("ssd", 0),
    ("fw", 1),
    ("fc", 1),
    ("rc", 0),
    ("fw", 4),
    ("fw", 2),
    ("ssd", 1),
    ("ssd", 2),
    ("ssd", 3),
    ("rd", 1),
    ("sx",),
    ("gu", 1),
    ("fw", 5),
    ("fc", 4),
    ("dn", 1),
    ("fc", 2),
    ("fw", 3),
    ("ch", 0),
    ("rd", 4),
    ("gu", 4),
    ("fw", 7),
    ("fc", 5),
    ("dn", 4),
    ("fc", 3),
    ("rd", 5),
    ("ch", 1),
    ("fw", 6),
    ("gu", 5),
    ("rc", 4),
    ("dn", 5),
    ("rd", 2),
    ("gu", 2),
    ("fc", 6),
    ("ch", 2),
    ("rc", 5),
    ("dn", 2),
    ("fc", 7),
    ("ry", 4),
    ("rd", 6),
    ("gu", 6),
    ("rc", 2),
    ("dn", 6),
    ("rd", 7),
    ("ch", 3),
    ("ry", 0),
    ("ry", 5),
    ("gu", 7),
    ("dn", 7),
    ("rc", 6),
    ("cb", 0),
    ("rc", 7),
    ("lr",),
    ("gn",),
    ("ry", 2),
    ("pj",),
    ("rc", 1),
    ("ry", 6),
    ("ry", 7),
    ("mc",),
    ("ry", 1),
    ("cb", 2),
    ("cb", 4),
    ("cb", 1),
    ("cb", 7),
    ("cb", 5),
    ("my",),
    ("cb", 6),
)


def silu(v):
    return v / (1.0 + jnp.exp(-v))


def dot(a, b):
    return jnp.dot(a, b, preferred_element_type=F32)


def dot_last(a, b, precision=None):
    return lax.dot_general(
        a, b, (((1,), (1,)), ((), ())), preferred_element_type=F32, precision=precision
    )


def widen(per_head, first, count, rows):
    lane = lax.broadcasted_iota(jnp.int32, (rows, LANES), 1)
    pieces = []
    for h in range(first, first + count, 2):
        left = jnp.broadcast_to(per_head[:, h : h + 1], (rows, LANES))
        right = jnp.broadcast_to(per_head[:, h + 1 : h + 2], (rows, LANES))
        pieces.append(jnp.where(lane < HEAD_DIM, left, right))
    return jnp.concatenate(pieces, axis=1)


def layer_kernel(
    E,
    T,
    picks_h,
    coefs_h,
    act_h,
    bgain_h,
    x_h,
    b_h,
    c_h,
    kx_h,
    kb_h,
    kc_h,
    pre_h,
    extra_h,
    valve_h,
    again_h,
    wg_h,
    wu_h,
    wd_h,
    wr_h,
    offset_h,
    speed_h,
    bypass_h,
    outa_ref,
    outb_ref,
    picks_v,
    coefs_v,
    act_v,
    bgain_v,
    x_v,
    b_v,
    c_v,
    kx_v,
    kb_v,
    kc_v,
    pre_v,
    extra_v,
    valve_v,
    again_v,
    wg_v,
    wu_v,
    wd_v,
    wr_v,
    offset_s,
    speed_s,
    bypass_s,
    nb,
    out,
    out1,
    X,
    hid,
    tc,
    fc,
    own,
    ys,
    yr,
    fin,
    ret,
    acc,
    cols_v,
    rim,
    joined,
    ybuf,
    cc_v,
    grown_v,
    state,
    st16,
    peerst,
    dec_v,
    peerdec,
    chin,
    chout,
    enter,
    esend,
    normed,
    atc,
    afc,
    aown,
    ays,
    ayr,
    load_sem,
    sent,
    out_r,
    y_r,
    core_r,
    sum_r,
    ysum_r,
    ret_r,
    once_r,
    state_r,
):
    e = lax.axis_index("ep")
    t = lax.axis_index("tp")
    y = lax.div(t, 2)
    c = lax.rem(t, 2)
    NY = T // 2
    b = E // UNITS
    blocks = {first: (first * b, count * b) for first, count in GROUPS}
    units = {first: range(first, first + count) for first, count in GROUPS}
    tok, width = act_v.shape
    S = width // T
    C = out.shape[1]
    rows, channels = x_v.shape
    latent = b_v.shape[1]
    heads = pre_v.shape[0]
    groups = latent // STATE
    members = heads // groups
    wide = members * HEAD_DIM
    taps = kx_v.shape[0]
    half = STATE // 2
    U = wg_v.shape[1]

    pairs = [
        (picks_h, picks_v),
        (coefs_h, coefs_v),
        (act_h, act_v),
        (bgain_h, bgain_v),
        (x_h, x_v),
        (b_h, b_v),
        (c_h, c_v),
        (kx_h, kx_v),
        (kb_h, kb_v),
        (kc_h, kc_v),
        (pre_h, pre_v),
        (extra_h, extra_v),
        (wg_h, wg_v),
        (wu_h, wu_v),
        (wd_h, wd_v),
        (valve_h, valve_v),
        (again_h, again_v),
        (wr_h, wr_v),
        (offset_h, offset_s),
        (speed_h, speed_s),
        (bypass_h, bypass_s),
    ]
    loads = {}
    for i, (src, dst) in enumerate(pairs):
        loads[i] = pltpu.make_async_copy(src, dst, load_sem.at[i])
        loads[i].start()

    def ep_peer(j):
        return (jnp.bitwise_xor(e, j), t)

    def y_peer(m):
        return (e, jnp.bitwise_xor(y, m) * 2 + c)

    core_peer = (e, y * 2 + 1 - c)

    barrier = pltpu.get_barrier_semaphore()
    peers = [ep_peer(j) for j in range(1, E)] + [y_peer(m) for m in range(1, NY)] + [core_peer]
    for peer in peers:
        pl.semaphore_signal(barrier, inc=1, device_id=peer, device_id_type=MESH)

    def rcopy(src, dst, ssem, rsem, dev):
        return pltpu.make_async_remote_copy(
            src_ref=src,
            dst_ref=dst,
            send_sem=ssem,
            recv_sem=rsem,
            device_id=dev,
            device_id_type=MESH,
        )

    def send(src, dst, kind, rsem, dev):
        rcopy(src, dst, sent.at[KINDS.index(kind)], rsem, dev).start()

    def drain(kind, whole):
        rcopy(whole, whole, sent.at[KINDS.index(kind)], state_r.at[0], core_peer).wait_send()

    def arrive(dst, rsem):
        rcopy(dst, dst, sent.at[0], rsem, core_peer).wait_recv()

    index_of = {k: i for i, k in enumerate(blocks)}
    others = pl.ds(1, NY - 1)
    every = pl.ds(0, NY)

    with jax.named_scope("load_b"):
        for i in range(4):
            loads[i].wait()
    pick = jnp.bitwise_xor(picks_v[...], e)
    expert = lax.broadcasted_iota(jnp.int32, (E, tok), 0)
    row_i = lax.broadcasted_iota(jnp.int32, (tok, tok), 0)
    col_i = lax.broadcasted_iota(jnp.int32, (tok, tok), 1)
    before = (row_i < col_i).astype(BF16)
    hot0 = (expert == pick[0:1]).astype(F32)
    hot1 = (expert == pick[1:2]).astype(F32)
    cum0 = dot(hot0.astype(BF16), before)
    cum1 = dot(hot1.astype(BF16), before) + jnp.sum(hot0, axis=1, keepdims=True)
    rank0 = jnp.sum(hot0 * cum0, axis=0, keepdims=True)
    rank1 = jnp.sum(hot1 * cum1, axis=0, keepdims=True)
    slot0 = pick[0:1].astype(F32) * float(C) + rank0
    slot1 = pick[1:2].astype(F32) * float(C) + rank1
    stacked = jnp.concatenate(
        [slot0, slot1, coefs_v[...], jnp.zeros((4, tok), F32)], axis=0
    )
    cols_v[...] = stacked.T

    wide_act = act_v[...].astype(F32)
    scale = lax.rsqrt(jnp.mean(wide_act * wide_act, axis=1, keepdims=True) + NORM_EPS)
    nb[...] = (wide_act * scale * bgain_v[...].astype(F32)[None, :]).astype(BF16)

    def placing(j):
        slot = (lax.broadcasted_iota(jnp.int32, (C, tok), 0) + j * C).astype(F32)
        return ((slot == slot0) | (slot == slot1)).astype(BF16)

    with jax.named_scope("load_a"):
        for i in range(4, 12):
            loads[i].wait()
    with jax.named_scope("barrier"):
        pl.semaphore_wait(barrier, len(peers))
    tail = pl.ds(rows - HALO, HALO)
    rims = [
        (x_v.at[tail], rim.at[:, pl.ds(0, channels)]),
        (b_v.at[tail], rim.at[:, pl.ds(channels, latent)]),
        (c_v.at[tail], rim.at[:, pl.ds(channels + latent, latent)]),
    ]
    following = (jnp.minimum(e + 1, E - 1), t)

    @pl.when(e < E - 1)
    def _():
        for src, dst in rims:
            send(src, dst, "rim", once_r.at[1], following)

    @pl.when(e == 0)
    def _():
        rim[...] = jnp.zeros(rim.shape, BF16)

    def normed_share(tt):
        return nb[:, pl.ds(pl.multiple_of(tt * S, S), S)]

    def share(m, cc):
        return jnp.bitwise_xor(y, m) * 2 + cc

    mine = normed_share(t)
    leaving = [j for unit in (0,) + SENDING for j in range(unit * b, unit * b + b) if j > 0]
    for j in leaving:
        u = j // b
        placed = placing(j)
        out[j] = dot(placed, mine).astype(BF16)
        send(out.at[j], X.at[t, j], "out", out_r.at[u], ep_peer(j))
        if u == TWICE:
            for m in range(1, NY):
                other = out1.at[m, j - TWICE * b]
                other[...] = dot(placed, normed_share(share(m, c))).astype(BF16)
                send(other, X.at[share(m, c), j], "out1", once_r.at[0], ep_peer(j))

    first = placing(0)
    for tt in range(T):
        X[tt, 0] = dot(first, nb[:, tt * S : (tt + 1) * S]).astype(BF16)

    def span(k):
        j0, n = blocks[k]
        return pl.ds(1, n - 1) if k == 0 else pl.ds(j0, n)

    def unit(u):
        return pl.ds(1, b - 1) if u == 0 else pl.ds(u * b, b)

    def local_only(k):
        return blocks[k][0] == 0 and blocks[k][1] == 1

    def forward(u):
        block = X.at[t, unit(u)]
        arrive(block, out_r.at[u])
        if u != TWICE:
            for m in range(1, NY):
                send(block, block, "y", y_r.at[u], y_peer(m))
        send(block, block, "core", core_r.at[u], core_peer)

    def forward_core(u):
        arrive(X.at[pl.ds(0, NY - 1), unit(u)], once_r.at[0] if u == TWICE else y_r.at[u])
        for m in range(1, NY):
            block = X.at[share(m, c), unit(u)]
            send(block, block, "core", core_r.at[u], core_peer)

    def ready(k):
        if k == 0 and b > 1:
            forward(0)
            forward_core(0)
        for u in units[k]:
            if u > 0 or b > 1:
                arrive(X.at[every, unit(u)], core_r.at[u])

    NT = min(512, U)
    NS = min(256, S)

    def span_rows(k):
        j0, n = blocks[k]
        return pl.ds(j0 * C, n * C)

    def gate_up(k):
        j0, n = blocks[k]

        def body(i, carry):
            at = pl.ds(pl.multiple_of(i * NT, NT), NT)
            gate = up = None
            for tt in range(T):
                r = X[tt, j0 : j0 + n].reshape(n * C, S)
                deep = slice(tt * S, (tt + 1) * S)
                g = dot(r, wg_v[deep, at])
                u = dot(r, wu_v[deep, at])
                gate = g if gate is None else gate + g
                up = u if up is None else up + u
            hid[0 : n * C, at] = (silu(gate) * up).astype(BF16)
            return carry

        lax.fori_loop(0, U // NT, body, 0)

    def down(k):
        rs = span_rows(k)
        size = blocks[k][1] * C
        for mine_side in (False, True):
            core = c if mine_side else 1 - c
            for m in list(range(1, NY)) + [0]:
                base = share(m, core) * S
                for n in range(S // NS):
                    at = pl.ds(pl.multiple_of(base + n * NS, NS), NS)
                    part = dot(hid[0:size], wd_v[:, at])
                    if mine_side:
                        own[m, rs, n * NS : (n + 1) * NS] = part
                    else:
                        tc[m, rs, n * NS : (n + 1) * NS] = part.astype(BF16)
                if not mine_side:
                    send(tc.at[m, rs], fc.at[m, rs], "tc", sum_r.at[index_of[k]], core_peer)

    def reduce_core(k):
        rs = span_rows(k)
        arrive(fc.at[every, rs], sum_r.at[index_of[k]])
        for m in list(range(1, NY)) + [0]:
            total = own[m, rs] + fc[m, rs].astype(F32)
            if m == 0:
                own[0, rs] = total
            else:
                ys[m, rs] = total.astype(BF16)
                send(ys.at[m, rs], yr.at[m, rs], "ys", ysum_r.at[index_of[k]], y_peer(m))

    def reduce_y(k):
        j0, n = blocks[k]
        rs = span_rows(k)
        total = own[0, rs]
        arrive(yr.at[others, rs], ysum_r.at[index_of[k]])
        for m in range(1, NY):
            total = total + yr[m, rs].astype(F32)
        done = total.astype(BF16).reshape(n, C, S)
        for i in range(n):
            j = j0 + i
            if j == 0:
                ret[0] = done[0]
            else:
                fin[j] = done[i]
                send(fin.at[j], ret.at[j], "fin", ret_r.at[index_of[k]], ep_peer(j))

    def combine(k, place):
        if not local_only(k):
            arrive(ret.at[span(k)], ret_r.at[index_of[k]])
        j0, n = blocks[k]
        size = n * C
        block = ret[j0 : j0 + n].reshape(size, S)
        lane = (lax.broadcasted_iota(jnp.int32, (tok, size), 1) + j0 * C).astype(F32)
        total = None
        for p in range(TOPK):
            chosen = (lane == cols_v[:, p : p + 1]).astype(BF16)
            term = dot(chosen, block) * cols_v[:, TOPK + p : TOPK + p + 1]
            total = term if total is None else total + term
        if place != "first":
            total = total + acc[...]
        if place != "last":
            acc[...] = total
        else:
            outb_ref[...] = total.astype(BF16)

    causal = row_i >= col_i

    def conv(ref, k_ref, start, size, rim_start):
        joined[0:HALO, 0:size] = rim[:, rim_start : rim_start + size].astype(F32)
        joined[HALO : HALO + rows, 0:size] = ref[:, start : start + size].astype(F32)
        kernel = k_ref[:, start : start + size].astype(F32)
        total = None
        for j in range(taps):
            at = HALO - taps + 1 + j
            term = kernel[j : j + 1] * joined[at : at + rows, 0:size]
            total = term if total is None else total + term
        return silu(total)

    def column(ref):
        index = lax.broadcasted_iota(jnp.int32, (heads, rows), 0)
        value = jnp.zeros((heads, rows), F32)
        for h in range(heads):
            value = jnp.where(index == h, ref[h], value)
        return value

    mix = {}
    lane128 = lax.broadcasted_iota(jnp.int32, (rows, LANES), 1)

    def mix_prepare():
        for i in (18, 19, 20):
            loads[i].wait()
        z = pre_v[...] + column(offset_s)
        step_t = jnp.maximum(z, 0.0) + jnp.log1p(jnp.exp(-jnp.abs(z)))
        decay_t = -jnp.exp(column(speed_s)) * step_t + extra_v[...]
        tri = causal.astype(F32)
        eye = (row_i == col_i).astype(F32)
        run = dot_last(tri, decay_t, HIGHEST)
        last = run[rows - 1 : rows]
        grown_v[...] = jnp.exp(run)
        dec_row = widen(jnp.exp(last), 0, heads, 1)
        dec_v[...] = jnp.broadcast_to(dec_row, dec_v.shape)
        mix["run"] = run
        mix["run_t"] = dot_last(decay_t, tri, HIGHEST)
        mix["step"] = dot_last(eye, step_t, HIGHEST)
        mix["to_end"] = jnp.exp(last - run)

    def ssd(g):
        run, run_t, step, to_end = (mix[n] for n in ("run", "run_t", "step", "to_end"))
        lead = g * members
        cols = slice(g * wide, (g + 1) * wide)
        xc = conv(x_v, kx_v, g * wide, wide, g * wide)
        bb = conv(b_v, kb_v, g * STATE, STATE, channels + g * STATE).astype(BF16)
        cc = conv(c_v, kc_v, g * STATE, STATE, channels + latent + g * STATE).astype(BF16)
        cc_v[:, g * STATE : (g + 1) * STATE] = cc
        xs = xc * widen(step, lead, members, rows)
        xs16 = xs.astype(BF16)
        scores = dot_last(cc, bb)
        scores = jnp.where(causal, scores, 0.0)
        inside = []
        skip = []
        for pair in range(0, members, 2):
            x_pair = xs16[:, pair * HEAD_DIM : (pair + 2) * HEAD_DIM]
            both = []
            for h in (lead + pair, lead + pair + 1):
                gap = jnp.minimum(run[:, h : h + 1] - run_t[h : h + 1, :], 0.0)
                weights = (jnp.exp(gap) * scores).astype(BF16)
                both.append(dot(weights, x_pair))
            inside.append(jnp.where(lane128 < HEAD_DIM, both[0], both[1]))
            h = lead + pair
            skip.append(jnp.where(lane128 < HEAD_DIM, bypass_s[h], bypass_s[h + 1]))
        ybuf[:, cols] = jnp.concatenate(inside, axis=1) + xc * jnp.concatenate(skip, axis=1)
        x_end = (xs * widen(to_end, lead, members, rows)).astype(BF16)
        state[:, cols] = lax.dot_general(
            bb, x_end, (((0,), (0,)), ((), ())), preferred_element_type=F32
        )

    side = lax.rem(e, 2)
    group = lax.div(e, 2)
    pairs_count = E // 2

    def state_exchange():
        st16[0] = state[0:half].astype(BF16)
        st16[1] = state[half:STATE].astype(BF16)
        send(st16.at[1 - side], peerst, "st16", state_r.at[0], ep_peer(1))
        send(dec_v, peerdec, "dec", state_r.at[1], ep_peer(1))

    behind = (jnp.maximum(e - 2, 0), t)
    ahead = (jnp.minimum(e + 2, E - 1), t)

    def chain(low, high):
        @pl.when((group >= low) & (group < high))
        def _():
            arrive(peerst, state_r.at[0])
            arrive(peerdec, state_r.at[1])
            own_half = st16[side].astype(F32)
            other = peerst[...].astype(F32)
            own_dec = dec_v[0:1]
            other_dec = peerdec[0:1]
            left = side == 0
            s0 = jnp.where(left, own_half, other)
            s1 = jnp.where(left, other, own_half)
            d0 = jnp.where(left, own_dec, other_dec)
            d1 = jnp.where(left, other_dec, own_dec)

            @pl.when(group > 0)
            def _():
                arrive(chin, state_r.at[2])

            @pl.when(group == 0)
            def _():
                chin[...] = jnp.zeros(chin.shape, BF16)

            e0 = chin[...].astype(F32)
            e1 = e0 * d0 + s0

            @pl.when(group < pairs_count - 1)
            def _():
                chout[...] = (e1 * d1 + s1).astype(BF16)
                send(chout, chin, "chain", state_r.at[2], ahead)

            enter[side] = jnp.where(left, e0, e1).astype(BF16)
            esend[...] = jnp.where(left, e1, e0).astype(BF16)
            send(esend, enter.at[side], "enter", state_r.at[3], ep_peer(1))

    def gate_norm():
        arrive(enter.at[1 - side], state_r.at[3])
        entered = enter[...].reshape(STATE, channels)
        for g in range(groups):
            cols = slice(g * wide, (g + 1) * wide)
            carried = dot(cc_v[:, g * STATE : (g + 1) * STATE], entered[:, cols])
            ssd_out = ybuf[:, cols] + carried * widen(grown_v[...], g * members, members, rows)
            gated = ssd_out * silu(valve_v[:, cols].astype(F32))
            norm = lax.rsqrt(jnp.mean(gated * gated, axis=1, keepdims=True) + NORM_EPS)
            normed[:, cols] = (gated * norm * again_v[cols].astype(F32)[None, :]).astype(BF16)

    width_a = wr_v.shape[1]
    NA = min(512, width_a)
    R = rows // T

    def project():
        for n in range(width_a // NA):
            part = dot(normed[...], wr_v[:, n * NA : (n + 1) * NA])
            for yy in range(NY):
                m = jnp.bitwise_xor(y, yy)
                low = part[(yy * 2) * R : (yy * 2 + 1) * R]
                high = part[(yy * 2 + 1) * R : (yy * 2 + 2) * R]
                aown[m, :, n * NA : (n + 1) * NA] = jnp.where(c == 0, low, high)
                atc[m, :, n * NA : (n + 1) * NA] = jnp.where(c == 0, high, low).astype(BF16)
        for m in list(range(1, NY)) + [0]:
            send(atc.at[m], afc.at[m], "atc", once_r.at[2], core_peer)

    def mix_core():
        arrive(afc, once_r.at[2])
        for m in list(range(1, NY)) + [0]:
            total = aown[m] + afc[m].astype(F32)
            if m == 0:
                aown[0] = total
            else:
                ays[m] = total.astype(BF16)
                send(ays.at[m], ayr.at[m], "ays", once_r.at[3], y_peer(m))

    def mix_y():
        total = aown[0]
        arrive(ayr.at[others], once_r.at[3])
        for m in range(1, NY):
            total = total + ayr[m].astype(F32)
        outa_ref[...] = total.astype(BF16)

    bounds = [round(i * pairs_count / 4) for i in range(5)]
    seen = []

    def load_weights():
        for i in (12, 13):
            loads[i].wait()

    def load_down():
        loads[14].wait()

    def load_rest():
        for i in (15, 16, 17):
            loads[i].wait()

    def await_rim():
        @pl.when(e > 0)
        def _():
            arrive(rim, once_r.at[1])

    def ssd_part(i):
        if i == 0:
            await_rim()
        for g in range(i * groups // 4, (i + 1) * groups // 4):
            ssd(g)

    def chain_part(i):
        chain(bounds[i], bounds[i + 1])

    def combine_part(k):
        seen.append(k)
        place = "first" if len(seen) == 1 else "last" if len(seen) == len(blocks) else "add"
        combine(k, place)

    steps = {
        "fw": forward,
        "fc": forward_core,
        "rd": ready,
        "gu": gate_up,
        "dn": down,
        "rc": reduce_core,
        "ry": reduce_y,
        "cb": combine_part,
        "mp": mix_prepare,
        "ssd": ssd_part,
        "sx": state_exchange,
        "ch": chain_part,
        "lw": load_weights,
        "ld": load_down,
        "lr": load_rest,
        "gn": gate_norm,
        "pj": project,
        "mc": mix_core,
        "my": mix_y,
    }
    for name, *which in ORDER:
        with jax.named_scope(name + "".join(str(i) for i in which)):
            steps[name](*which)

    with jax.named_scope("drain"):
        far = E - 1
        drain("out", out.at[pl.ds(1, far)])
        if TWICE > 0:
            drain("out1", out1.at[others])
            far -= b
        drain("y", X.at[pl.ds(0, NY - 1), pl.ds(0, far)])
        drain("core", X.at[every, pl.ds(1, E - 1)])
        drain("tc", tc)
        drain("ys", ys.at[others])
        drain("fin", fin.at[pl.ds(1, E - 1)])
        drain("st16", peerst)
        drain("dec", dec_v)
        drain("enter", esend)
        drain("atc", atc)
        drain("ays", ays.at[others])

        @pl.when(e < E - 1)
        def _():
            drain("rim", rim)

        @pl.when(group < pairs_count - 1)
        def _():
            drain("chain", chout)


def hand_over(a_ref, b_ref, outa_ref, outb_ref, sem):
    copies = [
        pltpu.make_async_copy(a_ref, outa_ref, sem.at[0]),
        pltpu.make_async_copy(b_ref, outb_ref, sem.at[1]),
    ]
    for copy in copies:
        copy.start()
    for copy in copies:
        copy.wait()


def local(
    blender_incoming_features,
    entry_latent_matrix,
    exit_latent_matrix,
    unactivated_valve,
    presoftplus_strides,
    extra_attenuation,
    incoming_feature_kernel,
    entry_latent_kernel,
    exit_latent_kernel,
    stride_offset_vector,
    attenuation_speed_exponent,
    bypass_coef_vector,
    cluster_rescale_coefs,
    blender_result_matrix,
    latter_microbatch_activations,
    specialist_rescale_coefs,
    specialist_valve_matrix,
    specialist_expand_matrix,
    specialist_contract_matrix,
    specialist_picks,
    selected_specialist_coefs,
):
    E = lax.axis_size("ep")
    T = lax.axis_size("tp")
    NY = T // 2
    rows, channels = blender_incoming_features.shape
    latent = entry_latent_matrix.shape[1]
    heads = presoftplus_strides.shape[1]
    taps = incoming_feature_kernel.shape[0]
    wide = channels // (latent // STATE)
    half = STATE // 2
    tok, width = latter_microbatch_activations.shape
    S = width // T
    C = 3 * tok * TOPK // (2 * E)
    b = E // UNITS
    wg, wu, wd = specialist_valve_matrix[0], specialist_expand_matrix[0], specialist_contract_matrix[0]
    U = wg.shape[1]
    width_a = blender_result_matrix.shape[1]
    R = rows // T
    far = [
        specialist_picks.T,
        selected_specialist_coefs.T,
        latter_microbatch_activations,
        specialist_rescale_coefs,
        blender_incoming_features,
        entry_latent_matrix,
        exit_latent_matrix,
        incoming_feature_kernel,
        entry_latent_kernel,
        exit_latent_kernel,
        presoftplus_strides.T,
        extra_attenuation.T,
        unactivated_valve,
        cluster_rescale_coefs,
        wg,
        wu,
        wd,
        blender_result_matrix,
    ]
    near = [stride_offset_vector, attenuation_speed_exponent, bypass_coef_vector]
    landing = [pltpu.VMEM(a.shape, a.dtype) for a in far]
    landing += [pltpu.SMEM(a.shape, a.dtype) for a in near]
    dma = pltpu.SemaphoreType.DMA
    vmem = pltpu.VMEM
    mixed = pl.pallas_call(
        functools.partial(layer_kernel, E, T),
        in_specs=[pl.BlockSpec(memory_space=pl.ANY)] * len(far + near),
        out_specs=[pl.BlockSpec(memory_space=pltpu.VMEM)] * 2,
        out_shape=[pltpu.VMEM((R, width_a), BF16), pltpu.VMEM((tok, S), BF16)],
        scratch_shapes=landing
        + [
            vmem((tok, width), BF16),
            vmem((E, C, S), BF16),
            vmem((NY, b, C, S), BF16),
            vmem((T, E, C, S), BF16),
            vmem((max(n for _, n in GROUPS) * b * C, U), BF16),
            vmem((NY, E * C, S), BF16),
            vmem((NY, E * C, S), BF16),
            vmem((NY, E * C, S), F32),
            vmem((NY, E * C, S), BF16),
            vmem((NY, E * C, S), BF16),
            vmem((E, C, S), BF16),
            vmem((E, C, S), BF16),
            vmem((tok, S), F32),
            vmem((tok, 8), F32),
            vmem((HALO, channels + 2 * latent), BF16),
            vmem((rows + HALO, wide), F32),
            vmem((rows, channels), F32),
            vmem((rows, latent), BF16),
            vmem((rows, heads), F32),
            vmem((STATE, channels), F32),
            vmem((2, half, channels), BF16),
            vmem((half, channels), BF16),
            vmem((8, channels), F32),
            vmem((8, channels), F32),
            vmem((half, channels), BF16),
            vmem((half, channels), BF16),
            vmem((2, half, channels), BF16),
            vmem((half, channels), BF16),
            vmem((rows, channels), BF16),
            vmem((NY, R, width_a), BF16),
            vmem((NY, R, width_a), BF16),
            vmem((NY, R, width_a), F32),
            vmem((NY, R, width_a), BF16),
            vmem((NY, R, width_a), BF16),
            dma((len(far + near),)),
            dma((len(KINDS),)),
            dma((UNITS,)),
            dma((UNITS,)),
            dma((UNITS,)),
            dma((len(GROUPS),)),
            dma((len(GROUPS),)),
            dma((len(GROUPS),)),
            dma((4,)),
            dma((4,)),
        ],
        compiler_params=pltpu.CompilerParams(
            collective_id=0, has_side_effects=True, vmem_limit_bytes=60 * 1024 * 1024
        ),
        name="layer",
    )(*far, *near)
    mixed = [pltpu.with_memory_space_constraint(a, pltpu.VMEM) for a in mixed]
    return pl.pallas_call(
        hand_over,
        in_specs=[pl.BlockSpec(memory_space=pltpu.VMEM)] * 2,
        out_specs=[pl.BlockSpec(memory_space=pl.ANY)] * 2,
        out_shape=[jax.ShapeDtypeStruct(a.shape, a.dtype) for a in mixed],
        scratch_shapes=[dma((2,))],
        name="hand_over",
    )(*mixed)


def solution(mesh):
    in_specs = (
        P("ep", "tp"),
        P("ep", "tp"),
        P("ep", "tp"),
        P("ep", "tp"),
        P("ep", "tp"),
        P("ep", "tp"),
        P(None, "tp"),
        P(None, "tp"),
        P(None, "tp"),
        P("tp"),
        P("tp"),
        P("tp"),
        P("tp"),
        P("tp", None),
        P("ep", None),
        P(),
        P("ep", None, "tp"),
        P("ep", None, "tp"),
        P("ep", "tp", None),
        P("ep", None),
        P("ep", None),
    )
    out_specs = (P(("ep", "tp"), None), P("ep", "tp"))
    return jax.shard_map(local, mesh=mesh, in_specs=in_specs, out_specs=out_specs, check_vma=False)
```
